128 devices in a mesh: gr: 2 (over z_hi), fs: 32 (over z_lo, y, x), tp: 2 (over core).
Axes of the slice: x: 4, y: 4, z: 4 (z_hi: 2, z_lo: 2; z = z_hi * 2 + z_lo), core: 2. Of those that a mesh axis runs over, the one named last changes fastest.
Arguments:
- tokens: bfloat16 [65536, 3072], P(('gr', 'fs')), may hold values from -6 to 6
- norm_gain: float32 [3072], P(('gr', 'fs')), may hold values from 0.1 to 1.9
- gate_weight: float32 [32, 3072, 768], P(None, ('gr', 'fs'), 'tp'), may hold values from -0.109375 to 0.109375
- up_weight: float32 [32, 3072, 768], P(None, ('gr', 'fs'), 'tp'), may hold values from -0.109375 to 0.109375
- down_weight: float32 [32, 3072, 768], P(None, ('gr', 'fs'), 'tp'), may hold values from -0.21875 to 0.21875
- group_pick: int32 [65536], P(('gr', 'fs')), may hold values from 0 to 3, as said below
- expert_pick: int32 [65536, 2], P(('gr', 'fs')), may hold values from 0 to 7, as said below
- route_weight: float32 [65536, 2], P(('gr', 'fs')), may hold values from 0.1 to 1
Outputs:
- combined: bfloat16 [65536, 3072], P(('gr', 'fs'), 'tp')
- gate_served: bfloat16 [32, 3072, 768], P('fs', None, 'tp')
- up_served: bfloat16 [32, 3072, 768], P('fs', None, 'tp')
- down_served: bfloat16 [32, 3072, 768], P('fs', None, 'tp')
The draws below stay inside these ranges and needn't reach their ends.
Inputs may be any that keep to these rules, and one draw needn't show every extreme that they name: `group_pick`: in each aligned block of 1024 rows every group is picked by the same number of rows. `expert_pick`: the 2 entries of a row differ. In each aligned block of 1024 rows, every expert (group and number together) is named exactly 64 times.
All inputs are finite; a program needn't handle non-finite values.
Results may differ from the reference program's by a relative error of at most 0.0092.
Values may be sent and summed in bfloat16 or wider, within the bound.
A program may use at most 128 MiB of HBM per device.

```python
import math
import jax
import jax.numpy as jnp
from jax import lax

D = 3072
FF = 768
GROUPS = 4
TOP = 2
TOK_DEV = 1024
EXPERTS = 32
TOKENS = 65536
N_TP = 2


def routing(key):
    blocks = TOKENS // TOK_DEV
    per_group = EXPERTS // GROUPS
    position = jnp.arange(TOK_DEV, dtype=jnp.int32)
    group_of = position % GROUPS
    within = position // GROUPS
    first_pick = within % per_group
    second_pick = (first_pick + 1 + within // per_group % (per_group - 1)) % per_group

    def one_block(block_key):
        order_key, label_key = jax.random.split(block_key)
        order = jax.random.permutation(order_key, TOK_DEV)
        relabel = jax.vmap(lambda label_one: jax.random.permutation(label_one, per_group))(jax.random.split(label_key, GROUPS))
        first_label = relabel[group_of, first_pick]
        second_label = relabel[group_of, second_pick]
        pairs = jnp.stack([first_label, second_label], axis=1).astype(jnp.int32)
        group_tok = jnp.zeros((TOK_DEV,), jnp.int32).at[order].set(group_of)
        pair_tok = jnp.zeros((TOK_DEV, 2), jnp.int32).at[order].set(pairs)
        return (group_tok, pair_tok)
    block_keys = jax.random.split(jax.random.fold_in(key, 71), blocks)
    groups_all, pairs_all = jax.vmap(one_block)(block_keys)
    return (groups_all.reshape(TOKENS).astype(jnp.int32), pairs_all.reshape(TOKENS, 2).astype(jnp.int32))


def draw_group_pick(key, part):
    return routing(key)[0]


def draw_expert_pick(key, part):
    return routing(key)[1]


def block_levels(own_key, dims, pieces, low, high):
    def one(dim, shards_of):
        heights = jax.random.uniform(jax.random.fold_in(jax.random.fold_in(own_key, 6), dim), (shards_of,), jnp.float32, low / len(pieces), high / len(pieces))
        return jnp.repeat(jnp.exp(heights), dims[dim] // shards_of).reshape((-1,) + (1,) * (len(dims) - dim - 1))

    loudness = one(*pieces[0])
    for cut in pieces[1:]:
        loudness = loudness * one(*cut)
    return loudness


def centred(own_key, extent, spread, bound, pieces=(), held_as=jnp.bfloat16):
    result = jax.random.normal(own_key, extent, jnp.float32) * spread
    if len(pieces) > 0:
        result = block_levels(own_key, extent, pieces, -0.22, 0.18) * result
    return jnp.clip(result, min=-bound, max=bound).astype(held_as)


def setup_inputs(seed: int = 0) -> dict:
    key_of = jax.random.split(jax.random.key(seed), 9)
    return {
        "tokens": centred(key_of[0], (TOKENS, D), 1.0, 6.0, ((0, 64),)),
        "norm_gain": jnp.clip(1.0 + 0.18 * jax.random.normal(key_of[1], (D,), jnp.float32), 0.1, 1.9),
        "gate_weight": centred(key_of[2], (EXPERTS, D, FF), D ** -0.5, 0.109375, ((1, 64), (2, 2)), jnp.float32),
        "up_weight": centred(key_of[3], (EXPERTS, D, FF), D ** -0.5, 0.109375, ((1, 64), (2, 2)), jnp.float32),
        "down_weight": centred(key_of[4], (EXPERTS, D, FF), FF ** -0.5, 0.21875, ((1, 64), (2, 2)), jnp.float32),
        "group_pick": draw_group_pick(jax.random.fold_in(key_of[8], 71), 0),
        "expert_pick": draw_expert_pick(jax.random.fold_in(key_of[8], 71), 0),
        "route_weight": jnp.clip(jnp.exp(math.log(1.0) - 2.3025851 * jax.random.uniform(key_of[7], (TOKENS, TOP), jnp.float32) ** block_levels(key_of[7], (TOKENS, TOP), ((0, 64),), -0.2, 0.2)), 0.1, 1.0),
    }


EPS = 1e-06

def reference(tokens, norm_gain, gate_weight, up_weight, down_weight, group_pick, expert_pick, route_weight):
    gate_served = (norm_gain[None, :, None] * gate_weight).astype(jnp.bfloat16)
    up_served = (norm_gain[None, :, None] * up_weight).astype(jnp.bfloat16)
    down_served = down_weight.astype(jnp.bfloat16)
    as_float = tokens.astype(jnp.float32)
    normed = (as_float * lax.rsqrt(lax.optimization_barrier(jnp.mean(as_float * as_float, axis=-1, keepdims=True)) + EPS)).astype(jnp.bfloat16)
    expert_ids = (group_pick[:, None] * (EXPERTS // GROUPS) + expert_pick).reshape(-1).astype(jnp.int32)
    per_expert = TOP * TOKENS // EXPERTS
    half_width = FF // N_TP

    def run_expert(expert_item):
        w_gate, w_up, w_down, index = expert_item
        row_ids = jnp.nonzero(expert_ids == index, size=per_expert)[0]
        rows_in = normed[row_ids // TOP]
        gate_acts = jnp.dot(rows_in, w_gate, preferred_element_type=jnp.float32)
        up_acts = jnp.dot(rows_in, w_up, preferred_element_type=jnp.float32)
        hidden = (jax.nn.silu(gate_acts) * up_acts).astype(jnp.bfloat16)
        accum_sum = jnp.zeros((per_expert, D), jnp.float32)
        for block in range(N_TP):
            part_sum = lax.dot_general(hidden[:, block * half_width:(block + 1) * half_width], w_down[:, block * half_width:(block + 1) * half_width], (((1,), (1,)), ((), ())), preferred_element_type=jnp.float32)
            accum_sum = accum_sum + lax.optimization_barrier(part_sum.astype(jnp.bfloat16)).astype(jnp.float32)
        return (accum_sum.astype(jnp.bfloat16), row_ids)
    outputs, row_ids = lax.map(run_expert, (gate_served, up_served, down_served, jnp.arange(EXPERTS, dtype=jnp.int32)))
    flat_out = jnp.zeros((TOP * TOKENS, D), jnp.bfloat16).at[row_ids.reshape(-1)].set(outputs.reshape(-1, D))
    combined = lax.optimization_barrier(jnp.sum(route_weight[:, :, None] * flat_out.reshape(TOKENS, TOP, D).astype(jnp.float32), axis=1))
    return (combined.astype(jnp.bfloat16), gate_served, up_served, down_served)
```

```python
import functools

import jax
import jax.numpy as jnp
from jax import lax
from jax.experimental import pallas as pl
from jax.experimental.pallas import tpu as pltpu
from jax.sharding import PartitionSpec as P

GROUPS = 4
EPS = 1e-06
BF = jnp.bfloat16
F32 = jnp.float32


def sent_together(arrays, axis, split_dim, concat_dim, along):
    both = jnp.concatenate(arrays, axis=along)
    result, at, gathered = (
        lax.all_to_all(both, axis, split_axis=split_dim, concat_axis=concat_dim, tiled=True),
        0,
        [],
    )
    for a in arrays:
        gathered.append(lax.slice_in_dim(result, at, at + a.shape[along], axis=along))
        at += a.shape[along]
    return tuple(gathered)


def sent_together_2(arrays, axis, dim, along):
    both = jnp.concatenate(arrays, axis=along)
    result, at, gathered = (lax.all_gather(both, axis, axis=dim, tiled=True), 0, [])
    for a in arrays:
        gathered.append(lax.slice_in_dim(result, at, at + a.shape[along], axis=along))
        at += a.shape[along]
    return tuple(gathered)


def dispatch_kernel(experts, share, ids_ref, tok_ref, out_ref, tgt_ref, select, normed):
    rows = tok_ref.shape[0]
    width = out_ref.shape[1]
    step = pl.program_id(0)

    @pl.when(step == 0)
    def _():
        first = lax.axis_index("tp") * share
        ids0, ids1 = ids_ref[0:1, :], ids_ref[1:2, :]
        which = lax.broadcasted_iota(jnp.int32, (experts, rows), 0)
        named0, named1 = ids0 == which, ids1 == which
        named = named0 | named1
        before = (
            lax.broadcasted_iota(jnp.int32, (rows, rows), 0)
            < lax.broadcasted_iota(jnp.int32, (rows, rows), 1)
        )
        rank = jnp.dot(
            jnp.where(named, 1.0, 0.0).astype(BF),
            jnp.where(before, 1.0, 0.0).astype(BF),
            preferred_element_type=F32,
        )
        capacity = 2 * share
        rank0 = jnp.sum(jnp.where(named0, rank, 0.0), axis=0, keepdims=True)
        rank1 = jnp.sum(jnp.where(named1, rank, 0.0), axis=0, keepdims=True)
        tgt_ref[0:1, :] = ids0 * capacity + rank0.astype(jnp.int32)
        tgt_ref[1:2, :] = ids1 * capacity + rank1.astype(jnp.int32)
        own = jnp.where(named, rank, -1.0).astype(jnp.int32)
        slot = lax.broadcasted_iota(jnp.int32, (share, rows), 0) + first
        for e in range(experts):
            hit = own[e : e + 1, :] == slot
            select[e * share : (e + 1) * share, :] = jnp.where(hit, 1.0, 0.0).astype(BF)

        @pl.loop(0, rows // 64)
        def _(r):
            at = pl.ds(pl.multiple_of(r * 64, 64), 64)
            x = tok_ref[at, :].astype(F32)
            scale = lax.rsqrt(jnp.mean(x * x, axis=-1, keepdims=True) + EPS)
            normed[at, :] = (x * scale).astype(BF)

    cols = pl.ds(pl.multiple_of(step * width, width), width)
    out_ref[...] = jnp.dot(select[...], normed[:, cols], preferred_element_type=F32).astype(BF)


def dispatch(ids, tokens, experts, share):
    rows, width = tokens.shape
    block = 512
    return pl.pallas_call(
        functools.partial(dispatch_kernel, experts, share),
        grid=(width // block,),
        out_shape=(
            jax.ShapeDtypeStruct((experts * share, width), BF),
            jax.ShapeDtypeStruct((2, rows), jnp.int32),
        ),
        in_specs=[
            pl.BlockSpec((2, rows), lambda i: (0, 0)),
            pl.BlockSpec((rows, width), lambda i: (0, 0)),
        ],
        out_specs=(
            pl.BlockSpec((experts * share, block), lambda i: (0, i)),
            pl.BlockSpec((2, rows), lambda i: (0, 0)),
        ),
        scratch_shapes=[
            pltpu.VMEM((experts * share, rows), BF),
            pltpu.VMEM((rows, width), BF),
        ],
        compiler_params=pltpu.CompilerParams(vmem_limit_bytes=48 * 1024 * 1024),
        cost_estimate=pl.CostEstimate(
            flops=2 * experts * share * rows * width,
            bytes_accessed=4 * rows * width,
            transcendentals=0,
        ),
        name="dispatch",
    )(ids, tokens)


def combine_kernel(tgt_ref, w_ref, rows_ref, out_ref, mix):
    @pl.when(pl.program_id(0) == 0)
    def _():
        slots = mix.shape[1]
        tile = 128

        @pl.loop(0, mix.shape[0] // tile)
        def _(r):
            at = pl.ds(pl.multiple_of(r * tile, tile), tile)
            slot = lax.broadcasted_iota(jnp.int32, (tile, slots), 1)
            t, w = tgt_ref[at, :], w_ref[at, :]
            mix[at, :] = jnp.where(
                slot == t[:, 0:1], w[:, 0:1], jnp.where(slot == t[:, 1:2], w[:, 1:2], 0.0)
            ).astype(BF)

    out_ref[...] = jnp.dot(mix[...], rows_ref[...], preferred_element_type=F32).astype(BF)


def combine(targets, weights, returned):
    rows = targets.shape[0]
    slots, width = returned.shape
    block = 512
    return pl.pallas_call(
        combine_kernel,
        grid=(width // block,),
        out_shape=jax.ShapeDtypeStruct((rows, width), BF),
        in_specs=[
            pl.BlockSpec((rows, 2), lambda i: (0, 0)),
            pl.BlockSpec((rows, 2), lambda i: (0, 0)),
            pl.BlockSpec((slots, block), lambda i: (0, i)),
        ],
        out_specs=pl.BlockSpec((rows, block), lambda i: (0, i)),
        scratch_shapes=[pltpu.VMEM((rows, slots), BF)],
        compiler_params=pltpu.CompilerParams(vmem_limit_bytes=48 * 1024 * 1024),
        cost_estimate=pl.CostEstimate(
            flops=2 * rows * slots * width, bytes_accessed=4 * slots * width, transcendentals=0
        ),
        name="combine",
    )(targets, weights, returned)


def local(
    tokens, norm_gain, gate_weight, up_weight, down_weight, group_pick, expert_pick, route_weight
):
    scaled = norm_gain[None, :, None]
    gate_local = (scaled * gate_weight).astype(BF)
    up_local = (scaled * up_weight).astype(BF)
    down_local = down_weight.astype(BF)
    experts = gate_local.shape[0]
    relaid = sent_together((gate_local, up_local, down_local), "fs", 0, 1, 2)
    gate_new, up_new, down_new = sent_together_2((relaid[0], relaid[1], relaid[2]), "gr", 1, 0)
    tok_rows, model_width = tokens.shape
    per_group = experts // GROUPS
    top_count = expert_pick.shape[1]
    capacity = top_count * tok_rows // experts
    share = capacity // lax.axis_size("tp")
    ids = group_pick[None, :] * per_group + expert_pick.T
    my_share, targets = dispatch(ids, tokens, experts, share)
    landed = lax.all_to_all(
        my_share.reshape(experts, share, model_width), "fs", split_axis=0, concat_axis=1, tiled=True
    ).reshape(experts, share, model_width)
    arrived = lax.all_gather(landed, "tp", axis=1, tiled=True).reshape(-1, model_width)
    gate_acts = jnp.dot(arrived, gate_new[0], preferred_element_type=jnp.float32)
    up_acts = jnp.dot(arrived, up_new[0], preferred_element_type=jnp.float32)
    hidden = (jax.nn.silu(gate_acts) * up_acts).astype(BF)
    partial_value = lax.dot_general(
        hidden, down_new[0], (((1,), (1,)), ((), ())), preferred_element_type=jnp.float32
    ).astype(BF)
    summed = lax.psum_scatter(partial_value, "tp", scatter_dimension=1, tiled=True)
    returned = lax.all_to_all(summed, "fs", split_axis=0, concat_axis=0, tiled=True)
    combined = combine(targets.T, route_weight, returned)
    return (combined, gate_new, up_new, down_new)


def solution(mesh):
    in_specs = (
        P(("gr", "fs"), None),
        P(("gr", "fs")),
        P(None, ("gr", "fs"), "tp"),
        P(None, ("gr", "fs"), "tp"),
        P(None, ("gr", "fs"), "tp"),
        P(("gr", "fs")),
        P(("gr", "fs"), None),
        P(("gr", "fs"), None),
    )
    out_specs = (
        P(("gr", "fs"), "tp"),
        P("fs", None, "tp"),
        P("fs", None, "tp"),
        P("fs", None, "tp"),
    )
    return jax.shard_map(local, mesh=mesh, in_specs=in_specs, out_specs=out_specs, check_vma=False)
```

```python
import functools

import jax
import jax.numpy as jnp
from jax import lax
from jax.experimental import pallas as pl
from jax.experimental.pallas import tpu as pltpu
from jax.sharding import PartitionSpec as P

GROUPS = 4
EPS = 1e-06
BF = jnp.bfloat16
F32 = jnp.float32
MESH = pl.DeviceIdType.MESH
MIB = 1024 * 1024
DYS = (2, 1, 3, 0)


def place():
    fs = lax.axis_index("fs")
    fz, y, x = fs // 16, (fs // 4) % 4, fs % 4
    return lax.axis_index("gr") * 2 + fz, fz, y, x, lax.axis_index("tp")


def dispatch_kernel(experts, share, ids_ref, tok_ref, out_ref, tgt_ref, select, normed, own):
    rows = tok_ref.shape[0]
    width = out_ref.shape[1]
    step = pl.program_id(0)

    @pl.when(step == 0)
    def _():
        _, fz, y, x, core = place()
        ids0, ids1 = ids_ref[0:1, :], ids_ref[1:2, :]
        which = lax.broadcasted_iota(jnp.int32, (experts, rows), 0)
        named0, named1 = ids0 == which, ids1 == which
        named = named0 | named1
        before = (
            lax.broadcasted_iota(jnp.int32, (rows, rows), 0)
            < lax.broadcasted_iota(jnp.int32, (rows, rows), 1)
        )
        rank = jnp.dot(
            jnp.where(named, 1.0, 0.0).astype(BF),
            jnp.where(before, 1.0, 0.0).astype(BF),
            preferred_element_type=F32,
        )
        capacity = 2 * share

        def row_of(ids, named_k):
            at = jnp.sum(jnp.where(named_k, rank, 0.0), axis=0, keepdims=True).astype(jnp.int32)
            far = (ids >> 4) ^ fz
            dy = ((ids >> 2) - y) & 3
            dx = (ids - x) & 3
            slot = jnp.where(dy == 2, 0, jnp.where(dy == 1, 1, jnp.where(dy == 3, 2, 3)))
            return far * (experts // 2 * capacity) + (slot * 4 + dx) * capacity + at

        tgt_ref[0:1, :] = row_of(ids0, named0)
        tgt_ref[1:2, :] = row_of(ids1, named1)
        own[...] = jnp.where(named, rank, -1.0).astype(jnp.int32)
        line = lax.broadcasted_iota(jnp.int32, (share, rows), 0)
        half = share // 2
        slots = (line + core * share, line + jnp.where(line < half, 0, half) + core * half)
        for j, dy in enumerate(DYS):
            for dx in range(4):
                for dz in range(2):
                    e = ((fz + dz) % 2) * 16 + ((y + dy) % 4) * 4 + (x + dx) % 4
                    at = ((j * 4 + dx) * 2 + dz) * share
                    hit = own[pl.ds(e, 1), :] == slots[dz]
                    select[at : at + share, :] = jnp.where(hit, 1.0, 0.0).astype(BF)

        @pl.loop(0, rows // 64)
        def _(r):
            at = pl.ds(pl.multiple_of(r * 64, 64), 64)
            v = tok_ref[at, :].astype(F32)
            scale = lax.rsqrt(jnp.mean(v * v, axis=-1, keepdims=True) + EPS)
            normed[at, :] = (v * scale).astype(BF)

    cols = pl.ds(pl.multiple_of(step * width, width), width)
    out_ref[...] = jnp.dot(select[...], normed[:, cols], preferred_element_type=F32).astype(BF)


def dispatch(ids, tokens, experts, share):
    rows, width = tokens.shape
    block = 512
    return pl.pallas_call(
        functools.partial(dispatch_kernel, experts, share),
        grid=(width // block,),
        out_shape=(
            jax.ShapeDtypeStruct((experts * share, width), BF),
            jax.ShapeDtypeStruct((2, rows), jnp.int32),
        ),
        in_specs=[
            pl.BlockSpec((2, rows), lambda i: (0, 0)),
            pl.BlockSpec((rows, width), lambda i: (0, 0)),
        ],
        out_specs=(
            pl.BlockSpec((experts * share, block), lambda i: (0, i)),
            pl.BlockSpec((2, rows), lambda i: (0, 0)),
        ),
        scratch_shapes=[
            pltpu.VMEM((experts * share, rows), BF),
            pltpu.VMEM((rows, width), BF),
            pltpu.VMEM((experts, rows), jnp.int32),
        ],
        compiler_params=pltpu.CompilerParams(vmem_limit_bytes=48 * MIB),
        cost_estimate=pl.CostEstimate(
            flops=2 * experts * share * rows * width,
            bytes_accessed=4 * rows * width,
            transcendentals=0,
        ),
        name="dispatch",
    )(ids, tokens)


def combine_kernel(tgt_ref, w_ref, rows_ref, out_ref, mix):
    @pl.when(pl.program_id(0) == 0)
    def _():
        slots = mix.shape[1]
        tile = 128

        @pl.loop(0, mix.shape[0] // tile)
        def _(r):
            at = pl.ds(pl.multiple_of(r * tile, tile), tile)
            slot = lax.broadcasted_iota(jnp.int32, (tile, slots), 1)
            t, w = tgt_ref[at, :], w_ref[at, :]
            mix[at, :] = jnp.where(
                slot == t[:, 0:1], w[:, 0:1], jnp.where(slot == t[:, 1:2], w[:, 1:2], 0.0)
            ).astype(BF)

    out_ref[...] = jnp.dot(mix[...], rows_ref[...], preferred_element_type=F32).astype(BF)


def combine(targets, weights, returned):
    rows = targets.shape[0]
    slots, width = returned.shape
    block = 512
    return pl.pallas_call(
        combine_kernel,
        grid=(width // block,),
        out_shape=jax.ShapeDtypeStruct((rows, width), BF),
        in_specs=[
            pl.BlockSpec((rows, 2), lambda i: (0, 0)),
            pl.BlockSpec((rows, 2), lambda i: (0, 0)),
            pl.BlockSpec((slots, block), lambda i: (0, i)),
        ],
        out_specs=pl.BlockSpec((rows, block), lambda i: (0, i)),
        scratch_shapes=[pltpu.VMEM((rows, slots), BF)],
        compiler_params=pltpu.CompilerParams(vmem_limit_bytes=48 * MIB),
        cost_estimate=pl.CostEstimate(
            flops=2 * rows * slots * width, bytes_accessed=4 * slots * width, transcendentals=0
        ),
        name="combine",
    )(targets, weights, returned)


def exchange_kernel(
    ms, wg, wu, wd, ret, og, ou, od,
    wx, wy, wf, tx, ty, lha, lhb, ps, po, ra, rb, rz, rya, ryb, send, recv, here,
):
    z, fz, y, x, core = place()
    used = {"away": 0, "near": 0}
    sent, local_copies = [], []

    def device(dz=0, dy=0, dx=0, flip=False):
        at_z = (z + dz) % 4
        return {
            "gr": at_z // 2,
            "fs": (at_z % 2) * 16 + ((y + dy) % 4) * 4 + (x + dx) % 4,
            "tp": 1 - core if flip else core,
        }

    def remote(src, dst, **to):
        at = used["away"]
        used["away"] += 1
        c = pltpu.make_async_remote_copy(
            src_ref=src,
            dst_ref=dst,
            send_sem=send.at[at],
            recv_sem=recv.at[at],
            device_id=device(**to),
            device_id_type=MESH,
        )
        c.start()
        sent.append(c)
        return c

    def near(src, dst):
        at = used["near"]
        used["near"] += 1
        c = pltpu.make_async_copy(src, dst, here.at[at])
        c.start()
        return c

    barrier = pltpu.get_barrier_semaphore()
    peers = [{"flip": True}] + [{axis: d} for axis in ("dz", "dy", "dx") for d in (1, 2, 3)]
    for to in peers:
        pl.semaphore_signal(barrier, inc=1, device_id=device(**to), device_id_type=MESH)
    pl.semaphore_wait(barrier, len(peers))

    stacks = (wg, wu, wd)
    pieces = [(k, dz) for k in range(3) for dz in (1, 0)]
    wx_own, wx_in = [], []
    for p, (k, dz) in enumerate(pieces):
        ez = (fz + dz) % 2
        wx_own.append(near(stacks[k].at[ez, :, x], wx.at[p, x]))
        wx_in.append(
            [remote(stacks[k].at[ez, :, (x + dx) % 4], wx.at[p, x], dx=dx) for dx in (2, 1, 3)]
        )
    tx_own, tx_in = [], []
    for j in range(4):
        to = tx if j < 3 else ty
        tx_own.append(near(ms.at[j, 0], to.at[j, 0]))
        tx_in.append([remote(ms.at[j, dx], to.at[j, dx], dx=dx) for dx in (2, 1, 3)])

    wy_own, wy_in, wf_own, wf_in = [], [], [], []

    def weights_y(p):
        wx_own[p].wait()
        for c in wx_in[p]:
            c.wait_recv()
        wy_own.append(near(wx.at[p, :, y], wy.at[p, y]))
        wy_in.append(
            [remote(wx.at[p, :, (y + dy) % 4], wy.at[p, y], dy=dy) for dy in (2, 1, 3)]
        )

    def weights_z(p):
        k, dz = pieces[p]
        wy_own[p].wait()
        for c in wy_in[p]:
            c.wait_recv()
        if dz == 0:
            wf_own.append(near(wy.at[p], wf.at[k, z]))
        for d in (2,) if dz == 0 else (1, 3):
            wf_in.append(remote(wy.at[p], wf.at[k, z], dz=d))

    ty_in, a_own, a_in, bz_in, b_in = [], [], [], [], []

    def tokens_y(j):
        tx_own[j].wait()
        for c in tx_in[j]:
            c.wait_recv()
        ty_in.append(remote(tx.at[j], ty.at[j], dy=DYS[j]))

    def tokens_z(j):
        if j < 3:
            ty_in[j].wait_recv()
        else:
            tx_own[3].wait()
            for c in tx_in[3]:
                c.wait_recv()
        half = ty.shape[3] // 2
        bz_in.append(
            [
                remote(ty.at[j, :, 1, pl.ds(h * half, half)], lhb.at[j, h, :, core], dz=d)
                for h, d in ((0, 1), (1, 3))
            ]
        )
        a_in.append(remote(ty.at[j, :, 0], lha.at[j, :, core], flip=True))
        a_own.append(near(ty.at[j, :, 0], lha.at[j, :, core]))

    def tokens_b(j):
        for c in bz_in[j]:
            c.wait_recv()
        b_in.append(
            [remote(lhb.at[j, h, :, core], lhb.at[j, h, :, core], flip=True) for h in range(2)]
        )

    weights_y(0)
    for p in range(1, 6):
        weights_y(p)
        weights_z(p - 1)
    weights_z(5)
    tokens_y(0)
    tokens_y(1)
    tokens_z(0)
    tokens_y(2)
    for j in (1, 2, 3):
        tokens_z(j)

    for c in wf_own:
        c.wait()
    for c in wf_in:
        c.wait_recv()
    written = [near(wf.at[k], out) for k, out in enumerate((og, ou, od))]

    width = wf.shape[-1]
    depth = wf.shape[2] * wf.shape[3] * wf.shape[4]

    def expert(rows, i):
        v = rows.reshape(-1, rows.shape[-1])
        gate = jnp.dot(v, wf[0].reshape(4 * depth, width), preferred_element_type=F32)
        up = jnp.dot(v, wf[1].reshape(4 * depth, width), preferred_element_type=F32)
        hidden = (gate / (1.0 + jnp.exp(-gate)) * up).astype(BF)

        def part(at_z):
            return lax.dot_general(
                hidden,
                wf[2, at_z].reshape(depth, width),
                (((1,), (1,)), ((), ())),
                preferred_element_type=F32,
            ).astype(BF).reshape(ps.shape[1:-1] + (depth,))

        for s in range(2):
            ps[i % 2, :, :, :, s * depth : (s + 1) * depth] = part((1 - core) * 2 + s)
        c = remote(ps.at[i % 2], ra.at[i] if i < 4 else rb.at[i - 4], flip=True)
        for s in range(2):
            po[i % 2, :, :, :, s * depth : (s + 1) * depth] = part(core * 2 + s)
        return c

    parts = []
    ry_in, rz_in, out_in, out_own = {}, {}, [], []

    def along_x(rows_of, part, j):
        out_own.append(near(rows_of(0), ret.at[part, j, 0]))
        for dx in (2, 1, 3):
            out_in.append(remote(rows_of(dx), ret.at[part, j, dx], dx=4 - dx))

    def near_rows(ref, j):
        return lambda dx: ref.at[j, dx // 2, pl.ds((dx % 2) * 2, 2)]

    def far_rows(ref, j):
        return lambda dx: ref.at[j, :, dx]

    def finish(i):
        parts[i].wait_recv()
        ref, j = (ra, i) if i < 4 else (rb, i - 4)
        ref[j] = (ref[j].astype(F32) + po[i % 2].astype(F32)).astype(BF)
        if i >= 4:
            rz_in[j] = [remote(rb.at[j, h], rz.at[j, h], dz=d) for h, d in ((0, 3), (1, 1))]
        elif j < 3:
            ry_in[j] = remote(ra.at[j], rya.at[j], dy=4 - DYS[j])
        else:
            along_x(near_rows(ra, 3), 0, 3)

    def near_back(j):
        ry_in[j].wait_recv()
        along_x(near_rows(rya, j), 0, j)

    def far_back_y(j):
        for c in rz_in[j]:
            c.wait_recv()
        if j < 3:
            ry_in[4 + j] = remote(rz.at[j], ryb.at[j], dy=4 - DYS[j])
        else:
            along_x(far_rows(rz, 3), 1, 3)

    def far_back_x(j):
        ry_in[4 + j].wait_recv()
        along_x(far_rows(ryb, j), 1, j)

    for i in range(8):
        if i < 4:
            a_own[i].wait()
            a_in[i].wait_recv()
        else:
            for c in b_in[i - 4]:
                c.wait_recv()
        if i >= 2:
            parts[i - 2].wait_send()
        parts.append(expert(lha[i] if i < 4 else lhb[i - 4], i))
        if 3 <= i < 7:
            tokens_b(i - 3)
        if i >= 1:
            finish(i - 1)
        if 3 <= i < 6:
            near_back(i - 3)
    finish(7)
    far_back_y(0)
    far_back_y(1)
    far_back_x(0)
    far_back_y(2)
    far_back_y(3)
    far_back_x(1)
    far_back_x(2)
    for c in out_in:
        c.wait_recv()
    for c in out_own + written:
        c.wait()
    waited = [id(c) for c in parts[:6]]
    for c in sent:
        if id(c) not in waited:
            c.wait_send()


def exchange(mine, gate, up, down):
    share, model = mine.shape[-2:]
    rows, width = gate.shape[-2:]
    half = share // 2
    cols = model // 2
    hbm = pl.BlockSpec(memory_space=pl.ANY)
    served = jax.ShapeDtypeStruct((4, 4, 4, rows, width), BF)
    back = (2, 4, share, cols)
    return pl.pallas_call(
        exchange_kernel,
        out_shape=(jax.ShapeDtypeStruct((2, 4, 4, 2, share, cols), BF), served, served, served),
        in_specs=[hbm] * 4,
        out_specs=(hbm,) * 4,
        scratch_shapes=[
            pltpu.VMEM((6, 4, 4, rows, width), BF),
            pltpu.VMEM((6, 4, 4, rows, width), BF),
            pltpu.VMEM((3, 4, 4, 4, rows, width), BF),
            pltpu.VMEM((3, 4, 2, share, model), BF),
            pltpu.VMEM((4, 4, 2, share, model), BF),
            pltpu.VMEM((4, 4, 2, share, model), BF),
            pltpu.VMEM((4, 2, 4, 2, half, model), BF),
            pltpu.VMEM((2,) + back, BF),
            pltpu.VMEM((2,) + back, BF),
            pltpu.VMEM((4,) + back, BF),
            pltpu.VMEM((4,) + back, BF),
            pltpu.VMEM((4,) + back, BF),
            pltpu.VMEM((3,) + back, BF),
            pltpu.VMEM((3,) + back, BF),
            pltpu.SemaphoreType.DMA((128,)),
            pltpu.SemaphoreType.DMA((128,)),
            pltpu.SemaphoreType.DMA((48,)),
        ],
        compiler_params=pltpu.CompilerParams(
            collective_id=0, has_side_effects=True, vmem_limit_bytes=63 * MIB
        ),
        name="exchange",
    )(mine, gate, up, down)


def local(
    tokens, norm_gain, gate_weight, up_weight, down_weight, group_pick, expert_pick, route_weight
):
    experts, rows, width = gate_weight.shape
    scaled = norm_gain[None, :, None]
    split = (2, 4, 4, rows, width)
    gate = (scaled * gate_weight).astype(BF).reshape(split)
    up = (scaled * up_weight).astype(BF).reshape(split)
    down = down_weight.astype(BF).reshape(split)
    tok_rows, model_width = tokens.shape
    top_count = expert_pick.shape[1]
    capacity = top_count * tok_rows // experts
    share = capacity // 2
    ids = group_pick[None, :] * (experts // GROUPS) + expert_pick.T
    mine, targets = dispatch(ids, tokens, experts, share)
    returned, gate_new, up_new, down_new = exchange(
        mine.reshape(4, 4, 2, share, model_width), gate, up, down
    )
    combined = combine(
        targets.T, route_weight, returned.reshape(experts * capacity, model_width // 2)
    )
    whole = (1, model_width, width)
    return (combined, gate_new.reshape(whole), up_new.reshape(whole), down_new.reshape(whole))


def solution(mesh):
    in_specs = (
        P(("gr", "fs"), None),
        P(("gr", "fs")),
        P(None, ("gr", "fs"), "tp"),
        P(None, ("gr", "fs"), "tp"),
        P(None, ("gr", "fs"), "tp"),
        P(("gr", "fs")),
        P(("gr", "fs"), None),
        P(("gr", "fs"), None),
    )
    out_specs = (
        P(("gr", "fs"), "tp"),
        P("fs", None, "tp"),
        P("fs", None, "tp"),
        P("fs", None, "tp"),
    )
    return jax.shard_map(local, mesh=mesh, in_specs=in_specs, out_specs=out_specs, check_vma=False)
```

```python
import functools

import jax
import jax.numpy as jnp
from jax import lax
from jax.experimental import pallas as pl
from jax.experimental.pallas import tpu as pltpu
from jax.sharding import PartitionSpec as P

GROUPS = 4
EPS = 1e-06
BF = jnp.bfloat16
F32 = jnp.float32
MESH = pl.DeviceIdType.MESH
MIB = 1024 * 1024
DYS = (2, 1, 3, 0)


def place():
    fs = lax.axis_index("fs")
    fz, y, x = fs // 16, (fs // 4) % 4, fs % 4
    return lax.axis_index("gr") * 2 + fz, fz, y, x, lax.axis_index("tp")


def dispatch_kernel(experts, share, ids_ref, tok_ref, out_ref, tgt_ref, select, normed, own):
    rows = tok_ref.shape[0]
    width = out_ref.shape[1]
    step = pl.program_id(0)

    @pl.when(step == 0)
    def _():
        _, fz, y, x, core = place()
        ids0, ids1 = ids_ref[0:1, :], ids_ref[1:2, :]
        which = lax.broadcasted_iota(jnp.int32, (experts, rows), 0)
        named0, named1 = ids0 == which, ids1 == which
        named = named0 | named1
        before = (
            lax.broadcasted_iota(jnp.int32, (rows, rows), 0)
            < lax.broadcasted_iota(jnp.int32, (rows, rows), 1)
        )
        rank = jnp.dot(
            jnp.where(named, 1.0, 0.0).astype(BF),
            jnp.where(before, 1.0, 0.0).astype(BF),
            preferred_element_type=F32,
        )
        capacity = 2 * share

        def row_of(ids, named_k):
            at = jnp.sum(jnp.where(named_k, rank, 0.0), axis=0, keepdims=True).astype(jnp.int32)
            far = (ids >> 4) ^ fz
            dy = ((ids >> 2) - y) & 3
            dx = (ids - x) & 3
            half = at >> 5
            first = jnp.where(half == 0, dx, dy)
            then = jnp.where(half == 0, dy, dx)
            slot = jnp.where(then == 2, 0, jnp.where(then == 1, 1, jnp.where(then == 3, 2, 3)))
            block = ((far * 4 + slot) * 2 + half) * 4 + first
            return block * share + (at & (share - 1))

        tgt_ref[0:1, :] = row_of(ids0, named0)
        tgt_ref[1:2, :] = row_of(ids1, named1)
        own[...] = jnp.where(named, rank, -1.0).astype(jnp.int32)
        half = share // 2
        line = lax.broadcasted_iota(jnp.int32, (half, rows), 0) + core * half
        for h in range(2):
            for j, then in enumerate(DYS):
                for first in range(4):
                    dx, dy = (then, first) if h else (first, then)
                    for dz in range(2):
                        e = ((fz + dz) % 2) * 16 + ((y + dy) % 4) * 4 + (x + dx) % 4
                        at = (((h * 4 + j) * 4 + first) * 2 + dz) * half
                        hit = own[pl.ds(e, 1), :] == line + h * share
                        select[at : at + half, :] = jnp.where(hit, 1.0, 0.0).astype(BF)

        @pl.loop(0, rows // 64)
        def _(r):
            at = pl.ds(pl.multiple_of(r * 64, 64), 64)
            v = tok_ref[at, :].astype(F32)
            scale = lax.rsqrt(jnp.mean(v * v, axis=-1, keepdims=True) + EPS)
            normed[at, :] = (v * scale).astype(BF)

    cols = pl.ds(pl.multiple_of(step * width, width), width)
    out_ref[...] = jnp.dot(select[...], normed[:, cols], preferred_element_type=F32).astype(BF)


def dispatch(ids, tokens, experts, share):
    rows, width = tokens.shape
    block = 512
    return pl.pallas_call(
        functools.partial(dispatch_kernel, experts, share),
        grid=(width // block,),
        out_shape=(
            jax.ShapeDtypeStruct((experts * share, width), BF),
            jax.ShapeDtypeStruct((2, rows), jnp.int32),
        ),
        in_specs=[
            pl.BlockSpec((2, rows), lambda i: (0, 0)),
            pl.BlockSpec((rows, width), lambda i: (0, 0)),
        ],
        out_specs=(
            pl.BlockSpec((experts * share, block), lambda i: (0, i)),
            pl.BlockSpec((2, rows), lambda i: (0, 0)),
        ),
        scratch_shapes=[
            pltpu.VMEM((experts * share, rows), BF),
            pltpu.VMEM((rows, width), BF),
            pltpu.VMEM((experts, rows), jnp.int32),
        ],
        compiler_params=pltpu.CompilerParams(vmem_limit_bytes=48 * MIB),
        cost_estimate=pl.CostEstimate(
            flops=2 * experts * share * rows * width,
            bytes_accessed=4 * rows * width,
            transcendentals=0,
        ),
        name="dispatch",
    )(ids, tokens)


def combine_kernel(tgt_ref, w_ref, rows_ref, g_ref, u_ref, d_ref, out_ref, go, uo, do, mix):
    go[...], uo[...], do[...] = g_ref[...], u_ref[...], d_ref[...]

    @pl.when(pl.program_id(0) == 0)
    def _():
        slots = mix.shape[1]
        tile = 128

        @pl.loop(0, mix.shape[0] // tile)
        def _(r):
            at = pl.ds(pl.multiple_of(r * tile, tile), tile)
            slot = lax.broadcasted_iota(jnp.int32, (tile, slots), 1)
            t, w = tgt_ref[at, :], w_ref[at, :]
            mix[at, :] = jnp.where(
                slot == t[:, 0:1], w[:, 0:1], jnp.where(slot == t[:, 1:2], w[:, 1:2], 0.0)
            ).astype(BF)

    out_ref[...] = jnp.dot(mix[...], rows_ref[...], preferred_element_type=F32).astype(BF)


def combine(targets, weights, returned, served):
    rows = targets.shape[0]
    slots, width = returned.shape
    block = 512
    steps = width // block
    lump = pl.BlockSpec((served[0].shape[0] // steps, served[0].shape[1]), lambda i: (i, 0))
    return pl.pallas_call(
        combine_kernel,
        grid=(steps,),
        out_shape=[jax.ShapeDtypeStruct((rows, width), BF)]
        + [jax.ShapeDtypeStruct(a.shape, BF) for a in served],
        in_specs=[
            pl.BlockSpec((rows, 2), lambda i: (0, 0)),
            pl.BlockSpec((rows, 2), lambda i: (0, 0)),
            pl.BlockSpec((slots, block), lambda i: (0, i)),
            lump,
            lump,
            lump,
        ],
        out_specs=[pl.BlockSpec((rows, block), lambda i: (0, i)), lump, lump, lump],
        scratch_shapes=[pltpu.VMEM((rows, slots), BF)],
        compiler_params=pltpu.CompilerParams(vmem_limit_bytes=48 * MIB),
        cost_estimate=pl.CostEstimate(
            flops=2 * rows * slots * width, bytes_accessed=4 * slots * width, transcendentals=0
        ),
        name="combine",
    )(targets, weights, returned, *served)


def exchange_kernel(
    ms, wg, wu, wd, ret, og, ou, od,
    wx, wy, wf, tx, ty, lha, lhb, ps, po, ra, rb, rz, rya, ryb, send, recv, here,
):
    z, fz, y, x, core = place()
    used = {"away": 0, "near": 0}
    sent, local_copies = [], []

    def device(dz=0, dy=0, dx=0, flip=False):
        at_z = (z + dz) % 4
        return {
            "gr": at_z // 2,
            "fs": (at_z % 2) * 16 + ((y + dy) % 4) * 4 + (x + dx) % 4,
            "tp": 1 - core if flip else core,
        }

    def remote(src, dst, **to):
        at = used["away"]
        used["away"] += 1
        c = pltpu.make_async_remote_copy(
            src_ref=src,
            dst_ref=dst,
            send_sem=send.at[at],
            recv_sem=recv.at[at],
            device_id=device(**to),
            device_id_type=MESH,
        )
        c.start()
        sent.append(c)
        return c

    def near(src, dst):
        at = used["near"]
        used["near"] += 1
        c = pltpu.make_async_copy(src, dst, here.at[at])
        c.start()
        return c

    barrier = pltpu.get_barrier_semaphore()
    peers = [{"flip": True}] + [{axis: d} for axis in ("dz", "dy", "dx") for d in (1, 2, 3)]
    for to in peers:
        pl.semaphore_signal(barrier, inc=1, device_id=device(**to), device_id_type=MESH)
    pl.semaphore_wait(barrier, len(peers))

    stacks = (wg, wu, wd)
    pieces = [(k, dz) for k in range(3) for dz in (1, 0)]
    wx_own, wx_in, wy_own, wy_in, wf_own, wf_in = [], [], [], [], [], []
    for p, (k, dz) in enumerate(pieces):
        stack = stacks[k].at[(fz + dz) % 2]
        wx_own.append(near(stack.at[:, x], wx.at[p, x]))
        wx_in.append([remote(stack.at[:, (x + d) % 4], wx.at[p, x], dx=d) for d in (2, 1, 3)])

    def weights_y(p):
        wx_own[p].wait()
        for c in wx_in[p]:
            c.wait_recv()
        wy_own.append(near(wx.at[p, :, y], wy.at[p, y]))
        wy_in.append([remote(wx.at[p, :, (y + d) % 4], wy.at[p, y], dy=d) for d in (2, 1, 3)])

    def weights_z(p):
        k, dz = pieces[p]
        wy_own[p].wait()
        for c in wy_in[p]:
            c.wait_recv()
        if dz == 0:
            wf_own.append(near(wy.at[p], wf.at[k, z]))
        for d in (2,) if dz == 0 else (1, 3):
            wf_in.append(remote(wy.at[p], wf.at[k, z], dz=d))

    axes = (("dx", "dy"), ("dy", "dx"))
    t1_own, t1_in, t2_in = {}, {}, {}
    a_own, a_in, bz_in, b_in = {}, {}, {}, {}

    def tokens_first(h, j):
        to = (tx if j < 3 else ty).at[h, j]
        t1_own[h, j] = near(ms.at[h, j, 0], to.at[0])
        t1_in[h, j] = [remote(ms.at[h, j, d], to.at[d], **{axes[h][0]: d}) for d in (2, 1, 3)]

    def tokens_second(h, j):
        t1_own[h, j].wait()
        for c in t1_in[h, j]:
            c.wait_recv()
        if j < 3:
            t2_in[h, j] = remote(tx.at[h, j], ty.at[h, j], **{axes[h][1]: DYS[j]})

    def tokens_third(j):
        for h in range(2):
            if j < 3:
                t2_in[h, j].wait_recv()
            bz_in[j, h] = remote(ty.at[h, j, :, 1], lhb.at[j, h, :, core], dz=1 + 2 * h)
            a_in[j, h] = remote(ty.at[h, j, :, 0], lha.at[j, h, :, core], flip=True)
            a_own[j, h] = near(ty.at[h, j, :, 0], lha.at[j, h, :, core])

    def tokens_b(j):
        for h in range(2):
            bz_in[j, h].wait_recv()
            b_in[j, h] = remote(lhb.at[j, h, :, core], lhb.at[j, h, :, core], flip=True)

    for j in range(4):
        tokens_first(0, j)
    weights_y(0)
    for p in range(1, 6):
        weights_y(p)
        weights_z(p - 1)
    for j in range(4):
        tokens_first(1, j)
    weights_z(5)
    for j in range(4):
        tokens_second(0, j)
        tokens_second(1, j)
    tokens_third(3)
    tokens_third(0)

    for c in wf_own:
        c.wait()
    for c in wf_in:
        c.wait_recv()
    written = [near(wf.at[k], out) for k, out in enumerate((og, ou, od))]

    width = wf.shape[-1]
    depth = wf.shape[2] * wf.shape[3] * wf.shape[4]

    parts = {}
    order = []

    def expert(far, j):
        for h in range(2):
            if far:
                b_in[j, h].wait_recv()
            else:
                a_own[j, h].wait()
                a_in[j, h].wait_recv()
        slot = len(order) % 2
        if len(order) >= 2:
            parts[order[-2]].wait_send()
        order.append((far, j))
        rows = lhb[j] if far else lha[j]
        v = rows.reshape(-1, rows.shape[-1])
        gate = jnp.dot(v, wf[0].reshape(4 * depth, width), preferred_element_type=F32)
        up = jnp.dot(v, wf[1].reshape(4 * depth, width), preferred_element_type=F32)
        hidden = (gate / (1.0 + jnp.exp(-gate)) * up).astype(BF)

        def part(at_z):
            return lax.dot_general(
                hidden,
                wf[2, at_z].reshape(depth, width),
                (((1,), (1,)), ((), ())),
                preferred_element_type=F32,
            ).astype(BF).reshape(ps.shape[1:-1] + (depth,))

        for s in range(2):
            ps[slot, :, :, :, s * depth : (s + 1) * depth] = part((1 - core) * 2 + s)
        parts[far, j] = remote(ps.at[slot], (rb if far else ra).at[j], flip=True)
        for s in range(2):
            po[slot, :, :, :, s * depth : (s + 1) * depth] = part(core * 2 + s)

    rq_in, rz_in, out_in, out_own = {}, {}, [], []

    def home(ref, far, j, h):
        out_own.append(near(ref.at[j, h, 0], ret.at[far, j, h, 0]))
        for d in (2, 1, 3):
            out_in.append(
                remote(ref.at[j, h, d], ret.at[far, j, h, d], **{axes[h][0]: 4 - d})
            )

    def second(ref, to, far, j, h):
        if j < 3:
            rq_in[far, j, h] = remote(ref.at[j, h], to.at[j, h], **{axes[h][1]: 4 - DYS[j]})
        else:
            home(ref, far, j, h)

    def finish(far, j):
        parts[far, j].wait_recv()
        ref = rb if far else ra
        slot = order.index((far, j)) % 2
        ref[j] = (ref[j].astype(F32) + po[slot].astype(F32)).astype(BF)
        for h in range(2):
            if far:
                rz_in[j, h] = remote(rb.at[j, h], rz.at[j, h], dz=3 - 2 * h)
            else:
                second(ra, rya, 0, j, h)

    def near_home(j):
        for h in range(2):
            rq_in[0, j, h].wait_recv()
            home(rya, 0, j, h)

    def far_second(j):
        for h in range(2):
            rz_in[j, h].wait_recv()
            second(rz, ryb, 1, j, h)

    def far_home(j):
        for h in range(2):
            rq_in[1, j, h].wait_recv()
            home(ryb, 1, j, h)

    expert(0, 3)
    expert(0, 0)
    finish(0, 3)
    finish(0, 0)
    tokens_third(1)
    tokens_third(2)
    tokens_b(0)
    expert(0, 1)
    expert(0, 2)
    finish(0, 1)
    expert(1, 0)
    finish(0, 2)
    finish(1, 0)
    near_home(0)
    tokens_b(1)
    tokens_b(2)
    expert(1, 1)
    expert(1, 2)
    finish(1, 1)
    tokens_b(3)
    finish(1, 2)
    near_home(1)
    near_home(2)
    far_second(0)
    expert(1, 3)
    finish(1, 3)
    far_second(1)
    far_second(2)
    far_home(0)
    far_second(3)
    far_home(1)
    far_home(2)
    for c in out_in:
        c.wait_recv()
    for c in out_own + written:
        c.wait()
    waited = [id(parts[key]) for key in order[:6]]
    for c in sent:
        if id(c) not in waited:
            c.wait_send()


def exchange(mine, gate, up, down):
    half, model = mine.shape[-2:]
    rows, width = gate.shape[-2:]
    cols = model // 2
    hbm = pl.BlockSpec(memory_space=pl.ANY)
    served = jax.ShapeDtypeStruct((4, 4, 4, rows, width), BF)
    back = (2, 4, 2 * half, cols)
    return pl.pallas_call(
        exchange_kernel,
        out_shape=(jax.ShapeDtypeStruct((2, 4) + back, BF), served, served, served),
        in_specs=[hbm] * 4,
        out_specs=(hbm,) * 4,
        scratch_shapes=[
            pltpu.VMEM((6, 4, 4, rows, width), BF),
            pltpu.VMEM((6, 4, 4, rows, width), BF),
            pltpu.VMEM((3, 4, 4, 4, rows, width), BF),
            pltpu.VMEM((2, 3, 4, 2, half, model), BF),
            pltpu.VMEM((2, 4, 4, 2, half, model), BF),
            pltpu.VMEM((4, 2, 4, 2, half, model), BF),
            pltpu.VMEM((4, 2, 4, 2, half, model), BF),
            pltpu.VMEM((2,) + back, BF),
            pltpu.VMEM((2,) + back, BF),
            pltpu.VMEM((4,) + back, BF),
            pltpu.VMEM((4,) + back, BF),
            pltpu.VMEM((4,) + back, BF),
            pltpu.VMEM((3,) + back, BF),
            pltpu.VMEM((3,) + back, BF),
            pltpu.SemaphoreType.DMA((180,)),
            pltpu.SemaphoreType.DMA((180,)),
            pltpu.SemaphoreType.DMA((64,)),
        ],
        compiler_params=pltpu.CompilerParams(
            collective_id=0, has_side_effects=True, vmem_limit_bytes=63 * MIB
        ),
        name="exchange",
    )(mine, gate, up, down)


def local(
    tokens, norm_gain, gate_weight, up_weight, down_weight, group_pick, expert_pick, route_weight
):
    experts, rows, width = gate_weight.shape
    scaled = norm_gain[None, :, None]
    split = (2, 4, 4, rows, width)
    gate = (scaled * gate_weight).astype(BF).reshape(split)
    up = (scaled * up_weight).astype(BF).reshape(split)
    down = down_weight.astype(BF).reshape(split)
    tok_rows, model_width = tokens.shape
    top_count = expert_pick.shape[1]
    capacity = top_count * tok_rows // experts
    share = capacity // 2
    ids = group_pick[None, :] * (experts // GROUPS) + expert_pick.T
    mine, targets = dispatch(ids, tokens, experts, share)
    returned, gate_new, up_new, down_new = exchange(
        mine.reshape(2, 4, 4, 2, share // 2, model_width), gate, up, down
    )
    served = [a.reshape(model_width, width) for a in (gate_new, up_new, down_new)]
    combined, *served = combine(
        targets.T, route_weight, returned.reshape(experts * capacity, model_width // 2), served
    )
    return (combined, *(a[None] for a in served))


def solution(mesh):
    in_specs = (
        P(("gr", "fs"), None),
        P(("gr", "fs")),
        P(None, ("gr", "fs"), "tp"),
        P(None, ("gr", "fs"), "tp"),
        P(None, ("gr", "fs"), "tp"),
        P(("gr", "fs")),
        P(("gr", "fs"), None),
        P(("gr", "fs"), None),
    )
    out_specs = (
        P(("gr", "fs"), "tp"),
        P("fs", None, "tp"),
        P("fs", None, "tp"),
        P("fs", None, "tp"),
    )
    return jax.shard_map(local, mesh=mesh, in_specs=in_specs, out_specs=out_specs, check_vma=False)
```

```python
import functools

import jax
import jax.numpy as jnp
from jax import lax
from jax.experimental import pallas as pl
from jax.experimental.pallas import tpu as pltpu
from jax.sharding import PartitionSpec as P

GROUPS = 4
EPS = 1e-06
BF = jnp.bfloat16
F32 = jnp.float32
MESH = pl.DeviceIdType.MESH
MIB = 1024 * 1024
DYS = (2, 1, 3, 0)


def place():
    fs = lax.axis_index("fs")
    fz, y, x = fs // 16, (fs // 4) % 4, fs % 4
    return lax.axis_index("gr") * 2 + fz, fz, y, x, lax.axis_index("tp")


def combine_kernel(table_ref, rows_ref, g_ref, u_ref, d_ref, out_ref, go, uo, do, mix, table):
    go[...], uo[...], do[...] = g_ref[...], u_ref[...], d_ref[...]

    @pl.when(pl.program_id(0) == 0)
    def _():
        slots = mix.shape[1]
        tile = 128
        table[...] = table_ref[...].T

        @pl.loop(0, mix.shape[0] // tile)
        def _(r):
            at = pl.ds(pl.multiple_of(r * tile, tile), tile)
            slot = lax.broadcasted_iota(jnp.int32, (tile, slots), 1)
            t = table[at, :]
            row = t.astype(jnp.int32)
            mix[at, :] = jnp.where(
                slot == row[:, 0:1], t[:, 2:3], jnp.where(slot == row[:, 1:2], t[:, 3:4], 0.0)
            ).astype(BF)

    out_ref[...] = jnp.dot(mix[...], rows_ref[...], preferred_element_type=F32).astype(BF)


def combine(table, returned, served):
    lines, rows = table.shape
    slots, width = returned.shape
    block = 512
    steps = width // block
    lump = pl.BlockSpec((served[0].shape[0] // steps, served[0].shape[1]), lambda i: (i, 0))
    return pl.pallas_call(
        combine_kernel,
        grid=(steps,),
        out_shape=[jax.ShapeDtypeStruct((rows, width), BF)]
        + [jax.ShapeDtypeStruct(a.shape, BF) for a in served],
        in_specs=[
            pl.BlockSpec((lines, rows), lambda i: (0, 0)),
            pl.BlockSpec((slots, block), lambda i: (0, i)),
            lump,
            lump,
            lump,
        ],
        out_specs=[pl.BlockSpec((rows, block), lambda i: (0, i)), lump, lump, lump],
        scratch_shapes=[pltpu.VMEM((rows, slots), BF), pltpu.VMEM((rows, lines), F32)],
        compiler_params=pltpu.CompilerParams(vmem_limit_bytes=63 * MIB),
        cost_estimate=pl.CostEstimate(
            flops=2 * rows * slots * width, bytes_accessed=4 * slots * width, transcendentals=0
        ),
        name="combine",
    )(table, returned, *served)


def exchange_kernel(
    group, picks, scales, tokens, wg, wu, wd, ret, og, ou, od, ms, table,
    wx, wy, wf, tx, ty, lha, lhb, ps, po, pool, select, own, stage, send, recv, here, ready,
):
    z, fz, y, x, core = place()
    ra, rb, rz, rya, ryb = (
        pool.at[pl.ds(at, n)] for at, n in ((0, 4), (4, 4), (8, 4), (12, 3), (15, 3))
    )
    used = {"away": 0, "near": 0}
    sent, local_copies = [], []

    def device(dz=0, dy=0, dx=0, flip=False):
        at_z = (z + dz) % 4
        return {
            "gr": at_z // 2,
            "fs": (at_z % 2) * 16 + ((y + dy) % 4) * 4 + (x + dx) % 4,
            "tp": 1 - core if flip else core,
        }

    def remote(src, dst, **to):
        at = used["away"]
        used["away"] += 1
        c = pltpu.make_async_remote_copy(
            src_ref=src,
            dst_ref=dst,
            send_sem=send.at[at],
            recv_sem=recv.at[at],
            device_id=device(**to),
            device_id_type=MESH,
        )
        c.start()
        sent.append(c)
        return c

    def near(src, dst):
        at = used["near"]
        used["near"] += 1
        c = pltpu.make_async_copy(src, dst, here.at[at])
        c.start()
        return c

    barrier = pltpu.get_barrier_semaphore()
    peers = [{"flip": True}] + [{axis: d} for axis in ("dz", "dy", "dx") for d in (1, 2, 3)]
    for to in peers:
        pl.semaphore_signal(barrier, inc=1, device_id=device(**to), device_id_type=MESH)
    pl.semaphore_wait(barrier, len(peers))

    stacks = (wg, wu, wd)
    pieces = [(k, dz) for k in range(3) for dz in (1, 0)]
    wx_own, wx_in, wy_own, wy_in, wf_own, wf_in = [], [], [], [], [], []
    for p, (k, dz) in enumerate(pieces):
        stack = stacks[k].at[(fz + dz) % 2]
        wx_own.append(near(stack.at[:, x], wx.at[p, x]))
        wx_in.append([remote(stack.at[:, (x + d) % 4], wx.at[p, x], dx=d) for d in (2, 1, 3)])

    cols = pool.shape[-1]
    loads = [
        near(tokens.at[b, :, :, :, pl.ds(s * cols, cols)], pool.at[s * 4 + b])
        for b in range(4)
        for s in range(2)
    ]

    def route():
        rows = group.shape[1]
        experts = own.shape[0]
        per_group = experts // GROUPS
        share = ms.shape[-2] * 2
        half = share // 2
        ids0 = group[...] * per_group + picks[0:1, :]
        ids1 = group[...] * per_group + picks[1:2, :]
        which = lax.broadcasted_iota(jnp.int32, (experts, rows), 0)
        named0, named1 = ids0 == which, ids1 == which
        named = named0 | named1
        before = (
            lax.broadcasted_iota(jnp.int32, (rows, rows), 0)
            < lax.broadcasted_iota(jnp.int32, (rows, rows), 1)
        )
        rank = jnp.dot(
            jnp.where(named, 1.0, 0.0).astype(BF),
            jnp.where(before, 1.0, 0.0).astype(BF),
            preferred_element_type=F32,
        )

        def row_of(ids, named_k):
            at = jnp.sum(jnp.where(named_k, rank, 0.0), axis=0, keepdims=True).astype(jnp.int32)
            far = (ids >> 4) ^ fz
            dy = ((ids >> 2) - y) & 3
            dx = (ids - x) & 3
            h = at >> 5
            first = jnp.where(h == 0, dx, dy)
            then = jnp.where(h == 0, dy, dx)
            slot = jnp.where(then == 2, 0, jnp.where(then == 1, 1, jnp.where(then == 3, 2, 3)))
            block = ((far * 4 + slot) * 2 + h) * 4 + first
            return (block * share + (at & (share - 1))).astype(F32)

        table[0:1, :] = row_of(ids0, named0)
        table[1:2, :] = row_of(ids1, named1)
        table[2:4, :] = scales[...]
        table[4:8, :] = jnp.zeros((4, rows), F32)
        own[...] = jnp.where(named, rank, -1.0).astype(jnp.int32)
        line = lax.broadcasted_iota(jnp.int32, (half, rows), 0) + core * half
        for h in range(2):
            for j, then in enumerate(DYS):
                for first in range(4):
                    dx, dy = (then, first) if h else (first, then)
                    for dz in range(2):
                        e = ((fz + dz) % 2) * 16 + ((y + dy) % 4) * 4 + (x + dx) % 4
                        at = (((h * 4 + j) * 4 + first) * 2 + dz) * half
                        hit = own[pl.ds(e, 1), :] == line + h * share
                        select[at : at + half, :] = jnp.where(hit, 1.0, 0.0).astype(BF)

    def normalize():
        for c in loads:
            c.wait()

        @pl.loop(0, 4)
        def _(b):
            for u in range(2):
                for w in range(2):
                    at = (u, pl.ds(w * 2, 2))
                    left = pool[(b,) + at].astype(F32)
                    right = pool[(4 + b,) + at].astype(F32)
                    total = jnp.sum(left * left, axis=-1, keepdims=True) + jnp.sum(
                        right * right, axis=-1, keepdims=True
                    )
                    scale = lax.rsqrt(total * (1.0 / (2 * cols)) + EPS)
                    pool[(b,) + at] = (left * scale).astype(BF)
                    pool[(4 + b,) + at] = (right * scale).astype(BF)

    placed = []
    block = stage.shape[-1]
    steps = cols // block

    def tile(t):
        s, n = t // steps, t % steps
        if t >= 2:
            placed[t - 2].wait()
        rows = pool[s * 4 : s * 4 + 4, :, :, :, n * block : (n + 1) * block]
        stage[t % 2] = (
            jnp.dot(select[...], rows.reshape(-1, block), preferred_element_type=F32)
            .astype(BF)
            .reshape(stage.shape[1:])
        )
        placed.append(
            near(stage.at[t % 2], ms.at[:, :, :, :, :, pl.ds(s * cols + n * block, block)])
        )

    def tokens_ready():
        for c in placed[-2:]:
            c.wait()
        for to in peers:
            pl.semaphore_signal(ready, inc=1, device_id=device(**to), device_id_type=MESH)

    def weights_y(p):
        wx_own[p].wait()
        for c in wx_in[p]:
            c.wait_recv()
        wy_own.append(near(wx.at[p, :, y], wy.at[p, y]))
        wy_in.append([remote(wx.at[p, :, (y + d) % 4], wy.at[p, y], dy=d) for d in (2, 1, 3)])

    def weights_z(p):
        k, dz = pieces[p]
        wy_own[p].wait()
        for c in wy_in[p]:
            c.wait_recv()
        if dz == 0:
            wf_own.append(near(wy.at[p], wf.at[k, z]))
        for d in (2,) if dz == 0 else (1, 3):
            wf_in.append(remote(wy.at[p], wf.at[k, z], dz=d))

    axes = (("dx", "dy"), ("dy", "dx"))
    t1_own, t1_in, t2_in = {}, {}, {}
    a_own, a_in, bz_in, b_in = {}, {}, {}, {}

    def tokens_first(h, j):
        to = (tx if j < 3 else ty).at[h, j]
        t1_own[h, j] = near(ms.at[h, j, 0], to.at[0])
        t1_in[h, j] = [remote(ms.at[h, j, d], to.at[d], **{axes[h][0]: d}) for d in (2, 1, 3)]

    def tokens_second(h, j):
        t1_own[h, j].wait()
        for c in t1_in[h, j]:
            c.wait_recv()
        if j < 3:
            t2_in[h, j] = remote(tx.at[h, j], ty.at[h, j], **{axes[h][1]: DYS[j]})

    def tokens_third(j):
        for h in range(2):
            if j < 3:
                t2_in[h, j].wait_recv()
            bz_in[j, h] = remote(ty.at[h, j, :, 1], lhb.at[j, h, :, core], dz=1 + 2 * h)
            a_in[j, h] = remote(ty.at[h, j, :, 0], lha.at[j, h, :, core], flip=True)
            a_own[j, h] = near(ty.at[h, j, :, 0], lha.at[j, h, :, core])

    def tokens_b(j):
        for h in range(2):
            bz_in[j, h].wait_recv()
            b_in[j, h] = remote(lhb.at[j, h, :, core], lhb.at[j, h, :, core], flip=True)

    route()
    normalize()
    tile(0)
    weights_y(0)
    tile(1)
    tile(2)
    weights_y(1)
    weights_z(0)
    tile(3)
    tile(4)
    weights_y(2)
    weights_z(1)
    tile(5)
    tokens_ready()
    for j in range(4):
        tokens_first(0, j)
    for p in range(3, 6):
        weights_y(p)
        weights_z(p - 1)
    for j in range(4):
        tokens_first(1, j)
    weights_z(5)
    for j in range(4):
        tokens_second(0, j)
        tokens_second(1, j)
    tokens_third(3)
    tokens_third(0)

    pl.semaphore_wait(ready, len(peers))
    for c in wf_own:
        c.wait()
    for c in wf_in:
        c.wait_recv()
    written = [near(wf.at[k], out) for k, out in enumerate((og, ou, od))]

    width = wf.shape[-1]
    depth = wf.shape[2] * wf.shape[3] * wf.shape[4]

    parts = {}
    order = []

    def expert(far, j):
        for h in range(2):
            if far:
                b_in[j, h].wait_recv()
            else:
                a_own[j, h].wait()
                a_in[j, h].wait_recv()
        slot = len(order) % 2
        if len(order) >= 2:
            parts[order[-2]].wait_send()
        order.append((far, j))
        rows = lhb[j] if far else lha[j]
        v = rows.reshape(-1, rows.shape[-1])
        gate = jnp.dot(v, wf[0].reshape(4 * depth, width), preferred_element_type=F32)
        up = jnp.dot(v, wf[1].reshape(4 * depth, width), preferred_element_type=F32)
        hidden = (gate / (1.0 + jnp.exp(-gate)) * up).astype(BF)

        def part(at_z):
            return lax.dot_general(
                hidden,
                wf[2, at_z].reshape(depth, width),
                (((1,), (1,)), ((), ())),
                preferred_element_type=F32,
            ).astype(BF).reshape(ps.shape[1:-1] + (depth,))

        for s in range(2):
            ps[slot, :, :, :, s * depth : (s + 1) * depth] = part((1 - core) * 2 + s)
        parts[far, j] = remote(ps.at[slot], (rb if far else ra).at[j], flip=True)
        for s in range(2):
            po[slot, :, :, :, s * depth : (s + 1) * depth] = part(core * 2 + s)

    rq_in, rz_in, out_in, out_own = {}, {}, [], []

    def home(ref, far, j, h):
        out_own.append(near(ref.at[j, h, 0], ret.at[far, j, h, 0]))
        for d in (2, 1, 3):
            out_in.append(
                remote(ref.at[j, h, d], ret.at[far, j, h, d], **{axes[h][0]: 4 - d})
            )

    def second(ref, to, far, j, h):
        if j < 3:
            rq_in[far, j, h] = remote(ref.at[j, h], to.at[j, h], **{axes[h][1]: 4 - DYS[j]})
        else:
            home(ref, far, j, h)

    def finish(far, j):
        parts[far, j].wait_recv()
        ref = rb if far else ra
        slot = order.index((far, j)) % 2
        ref[j] = (ref[j].astype(F32) + po[slot].astype(F32)).astype(BF)
        for h in range(2):
            if far:
                rz_in[j, h] = remote(rb.at[j, h], rz.at[j, h], dz=3 - 2 * h)
            else:
                second(ra, rya, 0, j, h)

    def near_home(j):
        for h in range(2):
            rq_in[0, j, h].wait_recv()
            home(rya, 0, j, h)

    def far_second(j):
        for h in range(2):
            rz_in[j, h].wait_recv()
            second(rz, ryb, 1, j, h)

    def far_home(j):
        for h in range(2):
            rq_in[1, j, h].wait_recv()
            home(ryb, 1, j, h)

    expert(0, 3)
    expert(0, 0)
    finish(0, 3)
    finish(0, 0)
    tokens_third(1)
    tokens_third(2)
    tokens_b(0)
    expert(0, 1)
    expert(0, 2)
    finish(0, 1)
    expert(1, 0)
    finish(0, 2)
    finish(1, 0)
    near_home(0)
    tokens_b(1)
    tokens_b(2)
    expert(1, 1)
    expert(1, 2)
    finish(1, 1)
    tokens_b(3)
    finish(1, 2)
    near_home(1)
    near_home(2)
    far_second(0)
    expert(1, 3)
    finish(1, 3)
    far_second(1)
    far_second(2)
    far_home(0)
    far_second(3)
    far_home(1)
    far_home(2)
    for c in out_in:
        c.wait_recv()
    for c in out_own + written:
        c.wait()
    waited = [id(parts[key]) for key in order[:6]]
    for c in sent:
        if id(c) not in waited:
            c.wait_send()


def exchange(group, picks, scales, tokens, gate, up, down):
    model = tokens.shape[-1]
    total = tokens.size // model
    rows, width = gate.shape[-2:]
    experts = gate.shape[0] * gate.shape[1] * gate.shape[2]
    half = picks.shape[0] * total // experts // 4
    cols = model // 2
    hbm = pl.BlockSpec(memory_space=pl.ANY)
    vmem = pl.BlockSpec(memory_space=pltpu.VMEM)
    served = jax.ShapeDtypeStruct((4, 4, 4, rows, width), BF)
    back = (2, 4, 2 * half, cols)
    return pl.pallas_call(
        exchange_kernel,
        out_shape=(
            jax.ShapeDtypeStruct((2, 4) + back, BF),
            served,
            served,
            served,
            jax.ShapeDtypeStruct((2, 4, 4, 2, half, model), BF),
            jax.ShapeDtypeStruct((8, total), F32),
        ),
        in_specs=[vmem] * 3 + [hbm] * 4,
        out_specs=(hbm,) * 5 + (vmem,),
        scratch_shapes=[
            pltpu.VMEM((6, 4, 4, rows, width), BF),
            pltpu.VMEM((6, 4, 4, rows, width), BF),
            pltpu.VMEM((3, 4, 4, 4, rows, width), BF),
            pltpu.VMEM((2, 3, 4, 2, half, model), BF),
            pltpu.VMEM((2, 4, 4, 2, half, model), BF),
            pltpu.VMEM((4, 2, 4, 2, half, model), BF),
            pltpu.VMEM((4, 2, 4, 2, half, model), BF),
            pltpu.VMEM((2,) + back, BF),
            pltpu.VMEM((2,) + back, BF),
            pltpu.VMEM((18,) + back, BF),
            pltpu.VMEM((experts * 2 * half, total), BF),
            pltpu.VMEM((experts, total), jnp.int32),
            pltpu.VMEM((2, 2, 4, 4, 2, half, 512), BF),
            pltpu.SemaphoreType.DMA((180,)),
            pltpu.SemaphoreType.DMA((180,)),
            pltpu.SemaphoreType.DMA((72,)),
            pltpu.SemaphoreType.REGULAR,
        ],
        compiler_params=pltpu.CompilerParams(
            collective_id=0, has_side_effects=True, vmem_limit_bytes=67_000_000
        ),
        name="exchange",
    )(group, picks, scales, tokens, gate, up, down)


def local(
    tokens, norm_gain, gate_weight, up_weight, down_weight, group_pick, expert_pick, route_weight
):
    experts, rows, width = gate_weight.shape
    scaled = norm_gain[None, :, None]
    split = (2, 4, 4, rows, width)
    gate = (scaled * gate_weight).astype(BF).reshape(split)
    up = (scaled * up_weight).astype(BF).reshape(split)
    down = down_weight.astype(BF).reshape(split)
    tok_rows, model_width = tokens.shape
    returned, gate_new, up_new, down_new, _, table = exchange(
        group_pick[None, :],
        expert_pick.T,
        route_weight.T,
        tokens.reshape(4, 2, 4, tok_rows // 32, model_width),
        gate,
        up,
        down,
    )
    served = [a.reshape(model_width, width) for a in (gate_new, up_new, down_new)]
    combined, *served = combine(
        table, returned.reshape(expert_pick.shape[1] * tok_rows, model_width // 2), served
    )
    return (combined, *(a[None] for a in served))


def solution(mesh):
    in_specs = (
        P(("gr", "fs"), None),
        P(("gr", "fs")),
        P(None, ("gr", "fs"), "tp"),
        P(None, ("gr", "fs"), "tp"),
        P(None, ("gr", "fs"), "tp"),
        P(("gr", "fs")),
        P(("gr", "fs"), None),
        P(("gr", "fs"), None),
    )
    out_specs = (
        P(("gr", "fs"), "tp"),
        P("fs", None, "tp"),
        P("fs", None, "tp"),
        P("fs", None, "tp"),
    )
    return jax.shard_map(local, mesh=mesh, in_specs=in_specs, out_specs=out_specs, check_vma=False)
```

```python
import functools

import jax
import jax.numpy as jnp
from jax import lax
from jax.experimental import pallas as pl
from jax.experimental.pallas import tpu as pltpu
from jax.sharding import PartitionSpec as P

GROUPS = 4
EPS = 1e-06
BF = jnp.bfloat16
F32 = jnp.float32
MESH = pl.DeviceIdType.MESH
MIB = 1024 * 1024
DYS = (2, 1, 3, 0)


def place():
    fs = lax.axis_index("fs")
    fz, y, x = fs // 16, (fs // 4) % 4, fs % 4
    return lax.axis_index("gr") * 2 + fz, fz, y, x, lax.axis_index("tp")


def combine_kernel(table_ref, rows_ref, g_ref, u_ref, d_ref, out_ref, go, uo, do, mix, table):
    go[...], uo[...], do[...] = g_ref[...], u_ref[...], d_ref[...]

    @pl.when(pl.program_id(0) == 0)
    def _():
        slots = mix.shape[1]
        tile = 128
        table[...] = table_ref[...].T

        @pl.loop(0, mix.shape[0] // tile)
        def _(r):
            at = pl.ds(pl.multiple_of(r * tile, tile), tile)
            slot = lax.broadcasted_iota(jnp.int32, (tile, slots), 1)
            t = table[at, :]
            row = t.astype(jnp.int32)
            mix[at, :] = jnp.where(
                slot == row[:, 0:1], t[:, 2:3], jnp.where(slot == row[:, 1:2], t[:, 3:4], 0.0)
            ).astype(BF)

    out_ref[...] = jnp.dot(mix[...], rows_ref[...], preferred_element_type=F32).astype(BF)


def combine(table, returned, served):
    lines, rows = table.shape
    slots, width = returned.shape
    block = 512
    steps = width // block
    lump = pl.BlockSpec((served[0].shape[0] // steps, served[0].shape[1]), lambda i: (i, 0))
    return pl.pallas_call(
        combine_kernel,
        grid=(steps,),
        out_shape=[jax.ShapeDtypeStruct((rows, width), BF)]
        + [jax.ShapeDtypeStruct(a.shape, BF) for a in served],
        in_specs=[
            pl.BlockSpec((lines, rows), lambda i: (0, 0)),
            pl.BlockSpec((slots, block), lambda i: (0, i)),
            lump,
            lump,
            lump,
        ],
        out_specs=[pl.BlockSpec((rows, block), lambda i: (0, i)), lump, lump, lump],
        scratch_shapes=[pltpu.VMEM((rows, slots), BF), pltpu.VMEM((rows, lines), F32)],
        compiler_params=pltpu.CompilerParams(vmem_limit_bytes=63 * MIB),
        cost_estimate=pl.CostEstimate(
            flops=2 * rows * slots * width, bytes_accessed=4 * slots * width, transcendentals=0
        ),
        name="combine",
    )(table, returned, *served)


def exchange_kernel(
    group, picks, scales, gain, tokens, wg, wu, wd, ret, og, ou, od, ms, table,
    wide, ws, wx, wy, wf, tx, ty, lha, lhb, ps, po, pool, own, send, recv, here, ready,
):
    z, fz, y, x, core = place()
    ra, rb, rz, rya = (
        pool.at[pl.ds(at, n)] for at, n in ((0, 4), (4, 4), (8, 4), (12, 3))
    )
    used = {"away": 0, "near": 0}
    sent, local_copies = [], []

    def device(dz=0, dy=0, dx=0, flip=False):
        at_z = (z + dz) % 4
        return {
            "gr": at_z // 2,
            "fs": (at_z % 2) * 16 + ((y + dy) % 4) * 4 + (x + dx) % 4,
            "tp": 1 - core if flip else core,
        }

    def remote(src, dst, **to):
        at = used["away"]
        used["away"] += 1
        c = pltpu.make_async_remote_copy(
            src_ref=src,
            dst_ref=dst,
            send_sem=send.at[at],
            recv_sem=recv.at[at],
            device_id=device(**to),
            device_id_type=MESH,
        )
        c.start()
        sent.append(c)
        return c

    def near(src, dst):
        at = used["near"]
        used["near"] += 1
        c = pltpu.make_async_copy(src, dst, here.at[at])
        c.start()
        return c

    stacks = (wg, wu, wd)
    pieces = [(k, dz) for k in range(3) for dz in (1, 0)]
    cast_order = (0, 4, 1, 5, 2, 3)
    wx_own, wx_in, wy_in, wf_own, wf_in = {}, {}, {}, [], []

    def fetch(q):
        k, dz = pieces[cast_order[q // 2]]
        return near(stacks[k].at[(fz + dz) % 2, pl.ds(q % 2 * 2, 2)], wide.at[q % 2])

    fetched = [fetch(0), fetch(1)]
    barrier = pltpu.get_barrier_semaphore()
    peers = [{"flip": True}] + [{axis: d} for axis in ("dz", "dy", "dx") for d in (1, 2, 3)]
    corners = [{"dy": i, "dx": j} for i in (1, 2, 3) for j in (1, 2, 3)]
    for to in peers + corners:
        pl.semaphore_signal(barrier, inc=1, device_id=device(**to), device_id_type=MESH)
    for i, p in enumerate(cast_order):
        k = pieces[p][0]
        for q in (2 * i, 2 * i + 1):
            fetched[q].wait()
            v = wide[q % 2]
            ws[p, q % 2 * 2 : q % 2 * 2 + 2] = (
                v if k == 2 else gain[...][None, None] * v
            ).astype(BF)
            if q + 2 < 2 * len(pieces):
                fetched.append(fetch(q + 2))
        if i == 0:
            pl.semaphore_wait(barrier, len(peers + corners))
        if p < 4:
            wx_own[p] = near(ws.at[p, :, x], wx.at[p, x])
            wx_in[p] = [remote(ws.at[p, :, (x + d) % 4], wx.at[p, x], dx=d) for d in (2, 1, 3)]
        else:
            wx_own[p] = near(ws.at[p, y], wx.at[p, y])
            wx_in[p] = [remote(ws.at[p, (y + d) % 4], wx.at[p, y], dy=d) for d in (2, 1, 3)]

    cols = pool.shape[-1]
    loads = [
        near(tokens.at[b, :, :, :, pl.ds(s * cols, cols)], pool.at[s * 4 + b])
        for b in range(4)
        for s in range(2)
    ]

    def route():
        rows = group.shape[1]
        experts = own.shape[0]
        per_group = experts // GROUPS
        share = ms.shape[-2]
        half = share // 2
        ids0 = group[...] * per_group + picks[0:1, :]
        ids1 = group[...] * per_group + picks[1:2, :]
        which = lax.broadcasted_iota(jnp.int32, (experts, rows), 0)
        named0, named1 = ids0 == which, ids1 == which
        named = named0 | named1
        counted = jnp.where(named, 1.0, 0.0).astype(BF)
        lump = 256
        rank = jnp.zeros(named.shape, F32)
        for at in range(0, rows, lump):
            before = (
                lax.broadcasted_iota(jnp.int32, (lump, rows), 0) + at
                < lax.broadcasted_iota(jnp.int32, (lump, rows), 1)
            )
            rank += jnp.dot(
                counted[:, at : at + lump],
                jnp.where(before, 1.0, 0.0).astype(BF),
                preferred_element_type=F32,
            )

        def row_of(ids, named_k):
            at = jnp.sum(jnp.where(named_k, rank, 0.0), axis=0, keepdims=True).astype(jnp.int32)
            far = (ids >> 4) ^ fz
            dy = ((ids >> 2) - y) & 3
            dx = (ids - x) & 3
            h = at >> 5
            first = jnp.where(h == 0, dx, dy)
            then = jnp.where(h == 0, dy, dx)
            slot = jnp.where(then == 2, 0, jnp.where(then == 1, 1, jnp.where(then == 3, 2, 3)))
            block = ((far * 4 + slot) * 2 + h) * 4 + first
            return (block * share + (at & (share - 1))).astype(F32)

        table[0:1, :] = row_of(ids0, named0)
        table[1:2, :] = row_of(ids1, named1)
        table[2:4, :] = scales[...]
        table[4:8, :] = jnp.zeros((4, rows), F32)
        own[...] = jnp.where(named, rank, -1.0).astype(jnp.int32)
        line = lax.broadcasted_iota(jnp.int32, (half, rows), 0) + core * half
        for h in range(2):
            for j, then in enumerate(DYS):
                for first in range(4):
                    dx, dy = (then, first) if h else (first, then)
                    for dz in range(2):
                        e = ((fz + dz) % 2) * 16 + ((y + dy) % 4) * 4 + (x + dx) % 4
                        at = (((h * 4 + j) * 4 + first) * 2 + dz) * half
                        hit = own[pl.ds(e, 1), :] == line + h * share
                        line_at = (at // 256 + 8, at // 128 % 2, at // 32 % 4, pl.ds(at % 32, half))
                        pool[line_at + (slice(0, rows),)] = jnp.where(hit, 1.0, 0.0).astype(BF)

    def normalize():
        for c in loads:
            c.wait()

        @pl.loop(0, 4)
        def _(b):
            for u in range(2):
                for w in range(2):
                    at = (u, pl.ds(w * 2, 2))
                    left = pool[(b,) + at].astype(F32)
                    right = pool[(4 + b,) + at].astype(F32)
                    total = jnp.sum(left * left, axis=-1, keepdims=True) + jnp.sum(
                        right * right, axis=-1, keepdims=True
                    )
                    scale = lax.rsqrt(total * (1.0 / (2 * cols)) + EPS)
                    pool[(b,) + at] = (left * scale).astype(BF)
                    pool[(4 + b,) + at] = (right * scale).astype(BF)

    placed = []

    def tile(t):
        s, m = t // 4, t % 4
        if t >= 2:
            placed[t - 2].wait()
        rows = pool[s * 4 : s * 4 + 4].reshape(-1, cols)
        select = pool[8 + m, :, :, :, : group.shape[1]].reshape(-1, group.shape[1])
        ps[t % 2] = (
            jnp.dot(select, rows, preferred_element_type=F32).astype(BF).reshape(ps.shape[1:])
        )
        to = ms.at[m // 2, pl.ds(m % 2 * 2, 2), :, :, pl.ds(s * cols, cols)]
        placed.append(near(ps.at[t % 2], to))

    def tokens_ready():
        for c in placed[-2:]:
            c.wait()
        for to in peers:
            pl.semaphore_signal(ready, inc=1, device_id=device(**to), device_id_type=MESH)

    def weights_up(p, block, at):
        k, dz = pieces[p]
        to = wf.at[k, z, at] if p < 4 else wf.at[k, z, :, at]
        if dz == 0:
            wf_own.append(near(block, to))
        for d in (2,) if dz == 0 else (1, 3):
            wf_in.append(remote(block, to, dz=d))

    def weights_y(p):
        wx_own[p].wait()
        for c in wx_in[p]:
            c.wait_recv()
        me, axis = (y, "dy") if p < 4 else (x, "dx")
        wy_in[p] = [
            remote(wx.at[p, :, (me + d) % 4], wy.at[p, me], **{axis: d}) for d in (2, 1, 3)
        ]
        weights_up(p, wx.at[p, :, me], me)

    def weights_z(p):
        me = y if p < 4 else x
        for d, c in zip((2, 1, 3), wy_in[p]):
            c.wait_recv()
            weights_up(p, wy.at[p, (me + 4 - d) % 4], (me + 4 - d) % 4)

    axes = (("dx", "dy"), ("dy", "dx"))
    t1_own, t1_in, t2_in = {}, {}, {}
    a_own, a_in, bz_in, b_in = {}, {}, {}, {}

    def tokens_first(h, j):
        to = (tx if j < 3 else ty).at[h, j]
        t1_own[h, j] = near(ms.at[h, j, 0], to.at[0])
        t1_in[h, j] = [remote(ms.at[h, j, d], to.at[d], **{axes[h][0]: d}) for d in (2, 1, 3)]

    def tokens_second(h, j):
        t1_own[h, j].wait()
        for c in t1_in[h, j]:
            c.wait_recv()
        if j < 3:
            t2_in[h, j] = remote(tx.at[h, j], ty.at[h, j], **{axes[h][1]: DYS[j]})

    def tokens_third(j):
        for h in range(2):
            if j < 3:
                t2_in[h, j].wait_recv()
            half = ty.shape[3] // 2
            near_half, far_half = (ty.at[h, j, :, pl.ds(i * half, half)] for i in range(2))
            bz_in[j, h] = remote(far_half, lhb.at[j, h, :, core], dz=1 + 2 * h)
            a_in[j, h] = remote(near_half, lha.at[j, h, :, core], flip=True)
            a_own[j, h] = near(near_half, lha.at[j, h, :, core])

    def tokens_b(j):
        for h in range(2):
            bz_in[j, h].wait_recv()
            b_in[j, h] = remote(lhb.at[j, h, :, core], lhb.at[j, h, :, core], flip=True)

    route()
    weights_y(0)
    weights_y(4)
    normalize()
    tile(0)
    tile(1)
    weights_y(1)
    weights_y(5)
    tile(2)
    tile(3)
    weights_z(0)
    weights_y(2)
    tile(4)
    tile(5)
    tile(6)
    weights_y(3)
    tile(7)
    tokens_ready()
    for j in (3, 0, 1, 2):
        for h in range(2):
            tokens_first(h, j)
    weights_z(1)
    weights_z(2)
    weights_z(4)
    weights_z(3)
    weights_z(5)
    tokens_second(0, 3)
    tokens_second(1, 3)
    tokens_third(3)
    for j in range(3):
        tokens_second(0, j)
        tokens_second(1, j)

    pl.semaphore_wait(ready, len(peers))
    for c in wf_own:
        c.wait()
    for c in wf_in:
        c.wait_recv()
    written = [near(wf.at[k], out) for k, out in enumerate((og, ou, od))]

    width = wf.shape[-1]
    depth = wf.shape[2] * wf.shape[3] * wf.shape[4]

    parts = {}
    order = []

    def expert(far, j):
        for h in range(2):
            if far:
                b_in[j, h].wait_recv()
            else:
                a_own[j, h].wait()
                a_in[j, h].wait_recv()
        slot = len(order) % 2
        if len(order) >= 2:
            parts[order[-2]].wait_send()
        order.append((far, j))
        rows = lhb[j] if far else lha[j]
        v = rows.reshape(-1, rows.shape[-1])
        gate = jnp.dot(v, wf[0].reshape(4 * depth, width), preferred_element_type=F32)
        up = jnp.dot(v, wf[1].reshape(4 * depth, width), preferred_element_type=F32)
        hidden = (gate / (1.0 + jnp.exp(-gate)) * up).astype(BF)

        def part(at_z):
            return lax.dot_general(
                hidden,
                wf[2, at_z].reshape(depth, width),
                (((1,), (1,)), ((), ())),
                preferred_element_type=F32,
            ).astype(BF).reshape(ps.shape[1:-1] + (depth,))

        for s in range(2):
            ps[slot, :, :, :, s * depth : (s + 1) * depth] = part((1 - core) * 2 + s)
        parts[far, j] = remote(ps.at[slot], (rb if far else ra).at[j], flip=True)
        for s in range(2):
            po[slot, :, :, :, s * depth : (s + 1) * depth] = part(core * 2 + s)

    rq_in, rz_in, out_in, out_own = {}, {}, [], []

    def home(ref, far, j, h):
        out_own.append(near(ref.at[j, h, 0], ret.at[far, j, h, 0]))
        for d in (2, 1, 3):
            out_in.append(
                remote(ref.at[j, h, d], ret.at[far, j, h, d], **{axes[h][0]: 4 - d})
            )

    def finish(far, j):
        parts[far, j].wait_recv()
        ref = rb if far else ra
        slot = order.index((far, j)) % 2
        ref[j] = (ref[j].astype(F32) + po[slot].astype(F32)).astype(BF)
        for h in range(2):
            if far:
                rz_in[j, h] = remote(rb.at[j, h], rz.at[j, h], dz=3 - 2 * h)
            elif j < 3:
                rq_in[j, h] = remote(ra.at[j, h], rya.at[j, h], **{axes[h][1]: 4 - DYS[j]})
            else:
                home(ra, 0, j, h)

    def near_home(j):
        for h in range(2):
            rq_in[j, h].wait_recv()
            home(rya, 0, j, h)

    def far_home(j):
        for h in range(2):
            rz_in[j, h].wait_recv()
            if j == 3:
                home(rz, 1, j, h)
                continue
            for d in (2, 1, 3, 0):
                to = {axes[h][0]: (4 - d) % 4, axes[h][1]: 4 - DYS[j]}
                out_in.append(remote(rz.at[j, h, d], ret.at[1, j, h, d], **to))

    expert(0, 3)
    tokens_third(0)
    expert(0, 0)
    finish(0, 3)
    finish(0, 0)
    tokens_third(1)
    tokens_third(2)
    tokens_b(0)
    expert(0, 1)
    expert(0, 2)
    finish(0, 1)
    expert(1, 0)
    finish(0, 2)
    finish(1, 0)
    near_home(0)
    tokens_b(1)
    tokens_b(2)
    expert(1, 1)
    near_home(1)
    near_home(2)
    expert(1, 2)
    finish(1, 1)
    tokens_b(3)
    finish(1, 2)
    far_home(0)
    expert(1, 3)
    finish(1, 3)
    far_home(1)
    far_home(2)
    far_home(3)
    for c in out_in:
        c.wait_recv()
    for c in out_own + written:
        c.wait()
    waited = [id(parts[key]) for key in order[:6]]
    for c in sent:
        if id(c) not in waited:
            c.wait_send()


def exchange(group, picks, scales, gain, tokens, gate, up, down):
    model = tokens.shape[-1]
    total = tokens.size // model
    rows, width = gate.shape[-2:]
    experts = gate.shape[0] * gate.shape[1] * gate.shape[2]
    half = picks.shape[0] * total // experts // 4
    cols = model // 2
    hbm = pl.BlockSpec(memory_space=pl.ANY)
    vmem = pl.BlockSpec(memory_space=pltpu.VMEM)
    served = jax.ShapeDtypeStruct((4, 4, 4, rows, width), BF)
    back = (2, 4, 2 * half, cols)
    return pl.pallas_call(
        exchange_kernel,
        out_shape=(
            jax.ShapeDtypeStruct((2, 4) + back, BF),
            served,
            served,
            served,
            jax.ShapeDtypeStruct((2, 4, 4, 2 * half, model), BF),
            jax.ShapeDtypeStruct((8, total), F32),
        ),
        in_specs=[vmem] * 4 + [hbm] * 4,
        out_specs=(hbm,) * 5 + (vmem,),
        scratch_shapes=[
            pltpu.VMEM((2, 2, 4, rows, width), F32),
            pltpu.VMEM((6, 4, 4, rows, width), BF),
            pltpu.VMEM((6, 4, 4, rows, width), BF),
            pltpu.VMEM((6, 4, 4, rows, width), BF),
            pltpu.VMEM((3, 4, 4, 4, rows, width), BF),
            pltpu.VMEM((2, 3, 4, 2 * half, model), BF),
            pltpu.VMEM((2, 4, 4, 2 * half, model), BF),
            pltpu.VMEM((4, 2, 4, 2, half, model), BF),
            pltpu.VMEM((4, 2, 4, 2, half, model), BF),
            pltpu.VMEM((2,) + back, BF),
            pltpu.VMEM((2,) + back, BF),
            pltpu.VMEM((15,) + back, BF),
            pltpu.VMEM((experts, total), jnp.int32),
            pltpu.SemaphoreType.DMA((216,)),
            pltpu.SemaphoreType.DMA((216,)),
            pltpu.SemaphoreType.DMA((88,)),
            pltpu.SemaphoreType.REGULAR,
        ],
        compiler_params=pltpu.CompilerParams(
            collective_id=0, has_side_effects=True, vmem_limit_bytes=67_000_000
        ),
        name="exchange",
    )(group, picks, scales, gain, tokens, gate, up, down)


def local(
    tokens, norm_gain, gate_weight, up_weight, down_weight, group_pick, expert_pick, route_weight
):
    experts, rows, width = gate_weight.shape
    split = (2, 4, 4, rows, width)
    tok_rows, model_width = tokens.shape
    returned, gate_new, up_new, down_new, _, table = exchange(
        group_pick[None, :],
        expert_pick.T,
        route_weight.T,
        norm_gain[:, None],
        tokens.reshape(4, 2, 4, tok_rows // 32, model_width),
        gate_weight.reshape(split),
        up_weight.reshape(split),
        down_weight.reshape(split),
    )
    served = [a.reshape(model_width, width) for a in (gate_new, up_new, down_new)]
    combined, *served = combine(
        table, returned.reshape(expert_pick.shape[1] * tok_rows, model_width // 2), served
    )
    return (combined, *(a[None] for a in served))


def solution(mesh):
    in_specs = (
        P(("gr", "fs"), None),
        P(("gr", "fs")),
        P(None, ("gr", "fs"), "tp"),
        P(None, ("gr", "fs"), "tp"),
        P(None, ("gr", "fs"), "tp"),
        P(("gr", "fs")),
        P(("gr", "fs"), None),
        P(("gr", "fs"), None),
    )
    out_specs = (
        P(("gr", "fs"), "tp"),
        P("fs", None, "tp"),
        P("fs", None, "tp"),
        P("fs", None, "tp"),
    )
    return jax.shard_map(local, mesh=mesh, in_specs=in_specs, out_specs=out_specs, check_vma=False)
```

```python
import functools

import jax
import jax.numpy as jnp
from jax import lax
from jax.experimental import pallas as pl
from jax.experimental.pallas import tpu as pltpu
from jax.sharding import PartitionSpec as P

GROUPS = 4
EPS = 1e-06
BF = jnp.bfloat16
F32 = jnp.float32
MESH = pl.DeviceIdType.MESH
MIB = 1024 * 1024
DYS = (2, 1, 3, 0)


def place():
    fs = lax.axis_index("fs")
    fz, y, x = fs // 16, (fs // 4) % 4, fs % 4
    return lax.axis_index("gr") * 2 + fz, fz, y, x, lax.axis_index("tp")


def combine_kernel(table_ref, rows_ref, g_ref, u_ref, d_ref, out_ref, go, uo, do, mix, table):
    go[...], uo[...], do[...] = g_ref[...], u_ref[...], d_ref[...]

    @pl.when(pl.program_id(0) == 0)
    def _():
        slots = mix.shape[1]
        tile = 128
        table[...] = table_ref[...].T

        @pl.loop(0, mix.shape[0] // tile)
        def _(r):
            at = pl.ds(pl.multiple_of(r * tile, tile), tile)
            slot = lax.broadcasted_iota(jnp.int32, (tile, slots), 1)
            t = table[at, :]
            row = t.astype(jnp.int32)
            mix[at, :] = jnp.where(
                slot == row[:, 0:1], t[:, 2:3], jnp.where(slot == row[:, 1:2], t[:, 3:4], 0.0)
            ).astype(BF)

    out_ref[...] = jnp.dot(mix[...], rows_ref[...], preferred_element_type=F32).astype(BF)


def combine(table, returned, served):
    lines, rows = table.shape
    slots, width = returned.shape
    block = 256
    steps = width // block
    lump = pl.BlockSpec((served[0].shape[0] // steps, served[0].shape[1]), lambda i: (i, 0))
    return pl.pallas_call(
        combine_kernel,
        grid=(steps,),
        out_shape=[jax.ShapeDtypeStruct((rows, width), BF)]
        + [jax.ShapeDtypeStruct(a.shape, BF) for a in served],
        in_specs=[
            pl.BlockSpec((lines, rows), lambda i: (0, 0)),
            pl.BlockSpec((slots, block), lambda i: (0, i)),
            lump,
            lump,
            lump,
        ],
        out_specs=[pl.BlockSpec((rows, block), lambda i: (0, i)), lump, lump, lump],
        scratch_shapes=[pltpu.VMEM((rows, slots), BF), pltpu.VMEM((rows, lines), F32)],
        compiler_params=pltpu.CompilerParams(vmem_limit_bytes=63 * MIB),
        cost_estimate=pl.CostEstimate(
            flops=2 * rows * slots * width, bytes_accessed=4 * slots * width, transcendentals=0
        ),
        name="combine",
    )(table, returned, *served)


def exchange_kernel(
    group, picks, scales, gain, tokens, wg, wu, wd, ret, og, ou, od, ms, table,
    wide, ws, wx, wy, wf, tx, ty, lha, lhb, ps, po, pool, own, send, recv, here, ready,
):
    z, fz, y, x, core = place()
    ra, rb, rz, rya = (
        pool.at[pl.ds(at, n)] for at, n in ((0, 4), (4, 4), (8, 4), (12, 3))
    )
    used = {"away": 0, "near": 0}
    sent, local_copies = [], []

    def device(dz=0, dy=0, dx=0, flip=False):
        at_z = (z + dz) % 4
        return {
            "gr": at_z // 2,
            "fs": (at_z % 2) * 16 + ((y + dy) % 4) * 4 + (x + dx) % 4,
            "tp": 1 - core if flip else core,
        }

    def remote(src, dst, **to):
        at = used["away"]
        used["away"] += 1
        c = pltpu.make_async_remote_copy(
            src_ref=src,
            dst_ref=dst,
            send_sem=send.at[at],
            recv_sem=recv.at[at],
            device_id=device(**to),
            device_id_type=MESH,
        )
        c.start()
        sent.append(c)
        return c

    def near(src, dst):
        at = used["near"]
        used["near"] += 1
        c = pltpu.make_async_copy(src, dst, here.at[at])
        c.start()
        return c

    stacks = (wg, wu, wd)
    pieces = [(k, dz) for k in range(3) for dz in (1, 0)]
    cast_order = (0, 4, 1, 5, 2, 3)
    wx_own, wx_in, wy_in, wf_own, wf_in = {}, {}, {}, [], []

    def fetch(q):
        k, dz = pieces[cast_order[q // 2]]
        return near(stacks[k].at[(fz + dz) % 2, pl.ds(q % 2 * 2, 2)], wide.at[q % 2])

    fetched = [fetch(0), fetch(1)]
    barrier = pltpu.get_barrier_semaphore()
    peers = [{"flip": True}] + [{axis: d} for axis in ("dz", "dy", "dx") for d in (1, 2, 3)]
    corners = [{"dy": i, "dx": j} for i in (1, 2, 3) for j in (1, 2, 3)]
    for to in peers + corners:
        pl.semaphore_signal(barrier, inc=1, device_id=device(**to), device_id_type=MESH)
    for i, p in enumerate(cast_order):
        k = pieces[p][0]
        for q in (2 * i, 2 * i + 1):
            fetched[q].wait()
            v = wide[q % 2]
            ws[p, q % 2 * 2 : q % 2 * 2 + 2] = (
                v if k == 2 else gain[...][None, None] * v
            ).astype(BF)
            if q + 2 < 2 * len(pieces):
                fetched.append(fetch(q + 2))
        if i == 0:
            pl.semaphore_wait(barrier, len(peers + corners))
        if p < 4:
            wx_own[p] = near(ws.at[p, :, x], wx.at[p, x])
            wx_in[p] = [remote(ws.at[p, :, (x + d) % 4], wx.at[p, x], dx=d) for d in (2, 1, 3)]
        else:
            wx_own[p] = near(ws.at[p, y], wx.at[p, y])
            wx_in[p] = [remote(ws.at[p, (y + d) % 4], wx.at[p, y], dy=d) for d in (2, 1, 3)]

    cols = pool.shape[-1]
    loads = [
        near(tokens.at[b, :, :, :, pl.ds(s * cols, cols)], pool.at[s * 4 + b])
        for b in range(4)
        for s in range(2)
    ]

    def route():
        rows = group.shape[1]
        experts = own.shape[0]
        per_group = experts // GROUPS
        share = ms.shape[-2]
        half = share // 2
        ids0 = group[...] * per_group + picks[0:1, :]
        ids1 = group[...] * per_group + picks[1:2, :]
        which = lax.broadcasted_iota(jnp.int32, (experts, rows), 0)
        named0, named1 = ids0 == which, ids1 == which
        named = named0 | named1
        counted = jnp.where(named, 1.0, 0.0).astype(BF)
        lump = 256
        rank = jnp.zeros(named.shape, F32)
        for at in range(0, rows, lump):
            before = (
                lax.broadcasted_iota(jnp.int32, (lump, rows), 0) + at
                < lax.broadcasted_iota(jnp.int32, (lump, rows), 1)
            )
            rank += jnp.dot(
                counted[:, at : at + lump],
                jnp.where(before, 1.0, 0.0).astype(BF),
                preferred_element_type=F32,
            )

        def row_of(ids, named_k):
            at = jnp.sum(jnp.where(named_k, rank, 0.0), axis=0, keepdims=True).astype(jnp.int32)
            far = (ids >> 4) ^ fz
            dy = ((ids >> 2) - y) & 3
            dx = (ids - x) & 3
            h = at >> 5
            first = jnp.where(h == 0, dx, dy)
            then = jnp.where(h == 0, dy, dx)
            slot = jnp.where(then == 2, 0, jnp.where(then == 1, 1, jnp.where(then == 3, 2, 3)))
            block = ((far * 4 + slot) * 2 + h) * 4 + first
            return (block * share + (at & (share - 1))).astype(F32)

        table[0:1, :] = row_of(ids0, named0)
        table[1:2, :] = row_of(ids1, named1)
        table[2:4, :] = scales[...]
        table[4:8, :] = jnp.zeros((4, rows), F32)
        own[...] = jnp.where(named, rank, -1.0).astype(jnp.int32)
        line = lax.broadcasted_iota(jnp.int32, (half, rows), 0) + core * half
        for h in range(2):
            for j, then in enumerate(DYS):
                for first in range(4):
                    dx, dy = (then, first) if h else (first, then)
                    for dz in range(2):
                        e = ((fz + dz) % 2) * 16 + ((y + dy) % 4) * 4 + (x + dx) % 4
                        at = (((h * 4 + j) * 4 + first) * 2 + dz) * half
                        hit = own[pl.ds(e, 1), :] == line + h * share
                        line_at = (at // 256 + 8, at // 128 % 2, at // 32 % 4, pl.ds(at % 32, half))
                        pool[line_at + (slice(0, rows),)] = jnp.where(hit, 1.0, 0.0).astype(BF)

    def normalize():
        for c in loads:
            c.wait()

        @pl.loop(0, 4)
        def _(b):
            for u in range(2):
                for w in range(2):
                    at = (u, pl.ds(w * 2, 2))
                    left = pool[(b,) + at].astype(F32)
                    right = pool[(4 + b,) + at].astype(F32)
                    total = jnp.sum(left * left, axis=-1, keepdims=True) + jnp.sum(
                        right * right, axis=-1, keepdims=True
                    )
                    scale = lax.rsqrt(total * (1.0 / (2 * cols)) + EPS)
                    pool[(b,) + at] = (left * scale).astype(BF)
                    pool[(4 + b,) + at] = (right * scale).astype(BF)

    placed = []

    def tile(t):
        s, m = t // 4, t % 4
        if t >= 2:
            placed[t - 2].wait()
        rows = pool[s * 4 : s * 4 + 4].reshape(-1, cols)
        select = pool[8 + m, :, :, :, : group.shape[1]].reshape(-1, group.shape[1])
        ps[t % 2] = (
            jnp.dot(select, rows, preferred_element_type=F32).astype(BF).reshape(ps.shape[1:])
        )
        to = ms.at[m // 2, pl.ds(m % 2 * 2, 2), :, :, pl.ds(s * cols, cols)]
        placed.append(near(ps.at[t % 2], to))

    def tokens_ready():
        for c in placed[-2:]:
            c.wait()
        for to in peers:
            pl.semaphore_signal(ready, inc=1, device_id=device(**to), device_id_type=MESH)

    def weights_up(p, block, at):
        k, dz = pieces[p]
        to = wf.at[k, z, at] if p < 4 else wf.at[k, z, :, at]
        if dz == 0:
            wf_own.append(near(block, to))
        for d in (2,) if dz == 0 else (1, 3):
            wf_in.append(remote(block, to, dz=d))

    def weights_y(p):
        wx_own[p].wait()
        for c in wx_in[p]:
            c.wait_recv()
        me, axis = (y, "dy") if p < 4 else (x, "dx")
        wy_in[p] = [
            remote(wx.at[p, :, (me + d) % 4], wy.at[p, me], **{axis: d}) for d in (2, 1, 3)
        ]
        weights_up(p, wx.at[p, :, me], me)

    def weights_z(p):
        me = y if p < 4 else x
        for d, c in zip((2, 1, 3), wy_in[p]):
            c.wait_recv()
            weights_up(p, wy.at[p, (me + 4 - d) % 4], (me + 4 - d) % 4)

    axes = (("dx", "dy"), ("dy", "dx"))
    t1_own, t1_in, t2_in = {}, {}, {}
    a_own, a_in, bz_in, b_in = {}, {}, {}, {}

    def tokens_first(h, j):
        to = (tx if j < 3 else ty).at[h, j]
        t1_own[h, j] = near(ms.at[h, j, 0], to.at[0])
        t1_in[h, j] = [remote(ms.at[h, j, d], to.at[d], **{axes[h][0]: d}) for d in (2, 1, 3)]

    def tokens_second(h, j):
        t1_own[h, j].wait()
        for c in t1_in[h, j]:
            c.wait_recv()
        if j < 3:
            t2_in[h, j] = remote(tx.at[h, j], ty.at[h, j], **{axes[h][1]: DYS[j]})

    def tokens_third(j):
        for h in range(2):
            if j < 3:
                t2_in[h, j].wait_recv()
            half = ty.shape[3] // 2
            near_half, far_half = (ty.at[h, j, :, pl.ds(i * half, half)] for i in range(2))
            bz_in[j, h] = remote(far_half, lhb.at[j, h, :, core], dz=1 + 2 * h)
            a_in[j, h] = remote(near_half, lha.at[j, h, :, core], flip=True)
            a_own[j, h] = near(near_half, lha.at[j, h, :, core])

    def tokens_b(j):
        for h in range(2):
            bz_in[j, h].wait_recv()
            b_in[j, h] = remote(lhb.at[j, h, :, core], lhb.at[j, h, :, core], flip=True)

    route()
    weights_y(0)
    weights_y(4)
    normalize()
    tile(0)
    tile(1)
    weights_y(1)
    weights_y(5)
    tile(2)
    tile(3)
    weights_z(0)
    weights_y(2)
    tile(4)
    tile(5)
    tile(6)
    weights_y(3)
    tile(7)
    tokens_ready()
    for j in (3, 0, 1, 2):
        for h in range(2):
            tokens_first(h, j)
    weights_z(1)
    weights_z(2)
    weights_z(4)
    weights_z(3)
    weights_z(5)
    tokens_second(0, 3)
    tokens_second(1, 3)
    tokens_third(3)
    for j in range(3):
        tokens_second(0, j)
        tokens_second(1, j)

    pl.semaphore_wait(ready, len(peers))
    for c in wf_own:
        c.wait()
    for c in wf_in:
        c.wait_recv()
    written = [near(wf.at[k], out) for k, out in enumerate((og, ou, od))]

    width = wf.shape[-1]
    depth = wf.shape[2] * wf.shape[3] * wf.shape[4]

    parts = {}
    order = []

    def expert(far, j):
        for h in range(2):
            if far:
                b_in[j, h].wait_recv()
            else:
                a_own[j, h].wait()
                a_in[j, h].wait_recv()
        slot = len(order) % 2
        if len(order) >= 2:
            parts[order[-2]].wait_send()
        order.append((far, j))
        rows = lhb[j] if far else lha[j]
        v = rows.reshape(-1, rows.shape[-1])
        gate = jnp.dot(v, wf[0].reshape(4 * depth, width), preferred_element_type=F32)
        up = jnp.dot(v, wf[1].reshape(4 * depth, width), preferred_element_type=F32)
        hidden = (gate / (1.0 + jnp.exp(-gate)) * up).astype(BF)

        def part(at_z):
            return lax.dot_general(
                hidden,
                wf[2, at_z].reshape(depth, width),
                (((1,), (1,)), ((), ())),
                preferred_element_type=F32,
            ).astype(BF).reshape(ps.shape[1:-1] + (depth,))

        for s in range(2):
            ps[slot, :, :, :, s * depth : (s + 1) * depth] = part((1 - core) * 2 + s)
        parts[far, j] = remote(ps.at[slot], (rb if far else ra).at[j], flip=True)
        for s in range(2):
            po[slot, :, :, :, s * depth : (s + 1) * depth] = part(core * 2 + s)

    rq_in, rz_in, out_in, out_own = {}, {}, [], []

    def home(ref, far, j, h):
        out_own.append(near(ref.at[j, h, 0], ret.at[far, j, h, 0]))
        for d in (2, 1, 3):
            out_in.append(
                remote(ref.at[j, h, d], ret.at[far, j, h, d], **{axes[h][0]: 4 - d})
            )

    def finish(far, j):
        parts[far, j].wait_recv()
        ref = rb if far else ra
        slot = order.index((far, j)) % 2
        ref[j] = (ref[j].astype(F32) + po[slot].astype(F32)).astype(BF)
        for h in range(2):
            if far:
                rz_in[j, h] = remote(rb.at[j, h], rz.at[j, h], dz=3 - 2 * h)
            elif j < 3:
                rq_in[j, h] = remote(ra.at[j, h], rya.at[j, h], **{axes[h][1]: 4 - DYS[j]})
            else:
                home(ra, 0, j, h)

    def near_home(j):
        for h in range(2):
            rq_in[j, h].wait_recv()
            home(rya, 0, j, h)

    def far_home(j):
        for h in range(2):
            rz_in[j, h].wait_recv()
            if j == 3:
                home(rz, 1, j, h)
                continue
            for d in (2, 1, 3, 0):
                to = {axes[h][0]: (4 - d) % 4, axes[h][1]: 4 - DYS[j]}
                out_in.append(remote(rz.at[j, h, d], ret.at[1, j, h, d], **to))

    expert(0, 3)
    tokens_third(0)
    expert(0, 0)
    finish(0, 3)
    finish(0, 0)
    tokens_third(1)
    tokens_third(2)
    tokens_b(0)
    expert(0, 1)
    expert(0, 2)
    finish(0, 1)
    expert(1, 0)
    finish(0, 2)
    finish(1, 0)
    near_home(0)
    tokens_b(1)
    tokens_b(2)
    expert(1, 1)
    near_home(1)
    near_home(2)
    expert(1, 2)
    finish(1, 1)
    tokens_b(3)
    finish(1, 2)
    far_home(0)
    expert(1, 3)
    finish(1, 3)
    far_home(1)
    far_home(2)
    far_home(3)
    for c in out_in:
        c.wait_recv()
    for c in out_own + written:
        c.wait()
    waited = [id(parts[key]) for key in order[:6]]
    for c in sent:
        if id(c) not in waited:
            c.wait_send()


def exchange(group, picks, scales, gain, tokens, gate, up, down):
    model = tokens.shape[-1]
    total = tokens.size // model
    rows, width = gate.shape[-2:]
    experts = gate.shape[0] * gate.shape[1] * gate.shape[2]
    half = picks.shape[0] * total // experts // 4
    cols = model // 2
    hbm = pl.BlockSpec(memory_space=pl.ANY)
    vmem = pl.BlockSpec(memory_space=pltpu.VMEM)
    served = jax.ShapeDtypeStruct((4, 4, 4, rows, width), BF)
    back = (2, 4, 2 * half, cols)
    return pl.pallas_call(
        exchange_kernel,
        out_shape=(
            jax.ShapeDtypeStruct((2, 4) + back, BF),
            served,
            served,
            served,
            jax.ShapeDtypeStruct((2, 4, 4, 2 * half, model), BF),
            jax.ShapeDtypeStruct((8, total), F32),
        ),
        in_specs=[vmem] * 4 + [hbm] * 4,
        out_specs=(hbm,) * 5 + (vmem,),
        scratch_shapes=[
            pltpu.VMEM((2, 2, 4, rows, width), F32),
            pltpu.VMEM((6, 4, 4, rows, width), BF),
            pltpu.VMEM((6, 4, 4, rows, width), BF),
            pltpu.VMEM((6, 4, 4, rows, width), BF),
            pltpu.VMEM((3, 4, 4, 4, rows, width), BF),
            pltpu.VMEM((2, 3, 4, 2 * half, model), BF),
            pltpu.VMEM((2, 4, 4, 2 * half, model), BF),
            pltpu.VMEM((4, 2, 4, 2, half, model), BF),
            pltpu.VMEM((4, 2, 4, 2, half, model), BF),
            pltpu.VMEM((2,) + back, BF),
            pltpu.VMEM((2,) + back, BF),
            pltpu.VMEM((15,) + back, BF),
            pltpu.VMEM((experts, total), jnp.int32),
            pltpu.SemaphoreType.DMA((216,)),
            pltpu.SemaphoreType.DMA((216,)),
            pltpu.SemaphoreType.DMA((88,)),
            pltpu.SemaphoreType.REGULAR,
        ],
        compiler_params=pltpu.CompilerParams(
            collective_id=0, has_side_effects=True, vmem_limit_bytes=67_000_000
        ),
        name="exchange",
    )(group, picks, scales, gain, tokens, gate, up, down)


def local(
    tokens, norm_gain, gate_weight, up_weight, down_weight, group_pick, expert_pick, route_weight
):
    experts, rows, width = gate_weight.shape
    split = (2, 4, 4, rows, width)
    tok_rows, model_width = tokens.shape
    returned, gate_new, up_new, down_new, _, table = exchange(
        group_pick[None, :],
        expert_pick.T,
        route_weight.T,
        norm_gain[:, None],
        tokens.reshape(4, 2, 4, tok_rows // 32, model_width),
        gate_weight.reshape(split),
        up_weight.reshape(split),
        down_weight.reshape(split),
    )
    served = [a.reshape(model_width, width) for a in (gate_new, up_new, down_new)]
    combined, *served = combine(
        table, returned.reshape(expert_pick.shape[1] * tok_rows, model_width // 2), served
    )
    return (combined, *(a[None] for a in served))


def solution(mesh):
    in_specs = (
        P(("gr", "fs"), None),
        P(("gr", "fs")),
        P(None, ("gr", "fs"), "tp"),
        P(None, ("gr", "fs"), "tp"),
        P(None, ("gr", "fs"), "tp"),
        P(("gr", "fs")),
        P(("gr", "fs"), None),
        P(("gr", "fs"), None),
    )
    out_specs = (
        P(("gr", "fs"), "tp"),
        P("fs", None, "tp"),
        P("fs", None, "tp"),
        P("fs", None, "tp"),
    )
    return jax.shard_map(local, mesh=mesh, in_specs=in_specs, out_specs=out_specs, check_vma=False)
```
